32 devices in a mesh: st: 8 (over z, x), tp: 4 (over y, core).
Axes of the slice: x: 2, y: 2, z: 4, core: 2. Of those that a mesh axis runs over, the one named last changes fastest.
Arguments:
- tokens: bfloat16 [4096, 2048], P('st'), may hold values from -6 to 6
- mix_query: bfloat16 [2048, 1024], P(None, 'tp'), may hold values from -0.125 to 0.125
- mix_key: bfloat16 [2048, 1024], P(None, 'tp'), may hold values from -0.125 to 0.125
- mix_value: bfloat16 [2048, 1024], P(None, 'tp'), may hold values from -0.125 to 0.125
- decay_lower_map: bfloat16 [2048, 64], replicated, may hold values from -0.125 to 0.125
- decay_upper_map: bfloat16 [64, 1024], P(None, 'tp'), may hold values from -1 to 1
- decay_base: float32 [1024], P('tp'), may hold values from -7.5 to -2.5
- decay_shift: float32 [4096, 16], P('st', 'tp'), may hold values from -3.8 to 9.8
- rate_lower_map: bfloat16 [2048, 64], replicated, may hold values from -0.125 to 0.125
- rate_upper_map: bfloat16 [64, 1024], P(None, 'tp'), may hold values from -0.75 to 0.75
- norm_gain: float32 [1024], P('tp'), may hold values from 0.1 to 1.9
- mix_out: bfloat16 [1024, 2048], P(None, 'tp'), may hold values from -0.1875 to 0.1875
- cross_query: bfloat16 [2048, 2048], P(None, 'tp'), may hold values from -0.125 to 0.125
- score_gain: float32 [2048], P('tp'), may hold values from 0.1 to 1.9
- passage_key: bfloat16 [2048, 2048], P(None, 'tp'), may hold values from -0.125 to 0.125
- passage_value: bfloat16 [2048, 2048], P(None, 'tp'), may hold values from -0.125 to 0.125
- cross_out: bfloat16 [2048, 2048], P(None, 'tp'), may hold values from -0.5 to 0.5
- gate_down: bfloat16 [2048, 128], replicated, may hold values from -0.125 to 0.125
- gate_up: bfloat16 [128, 2048], P(None, 'tp'), may hold values from -0.5 to 0.5
- store: bfloat16 [96, 96, 2048], P('st'), may hold values from -6 to 6
- passage_ids: int32 [64, 4], P('st'), may hold values from 0 to 95, as said below
Outputs:
- mixed: bfloat16 [4096, 2048], P('st', 'tp')
The draws below stay inside these ranges and needn't reach their ends.
Inputs may be any that keep to these rules, and one draw needn't show every extreme that they name: `passage_ids`: among the 32 passages named by the rows of one sequence, at most 4 are held by one index of st (passage p by index p // 12); in every draw exactly 4 are held by the index before the sequence's own.
All inputs are finite; a program needn't handle non-finite values.
Results may differ from the reference program's by a relative error of at most 0.0075.
Values may be sent and summed in bfloat16 or wider, within the bound.
No kernel may reach another device: no remote copies, remote signals or barrier semaphores. Data moves between devices by JAX's collectives and lax.ppermute only.
A program may use at most 128 MiB of HBM per device.

```python
import jax
import jax.numpy as jnp
from jax import lax

MODEL_DIM = 2048
MIXER_HEADS = 16
RHEAD = 64
XHEADS = 8
XHEAD = 256
LOWRANK_WIDTH = 64
GLORA = 128
PLEN = 96
PER_BLOCK = 4
QBLOCK = 64
MBLOCK = 64
TOKENS_PER_SEQ = 512
PASS_DEV = 12
MIXER_WIDTH = 1024
XWIDTH = 2048
TOKEN_TOTAL = 4096
NPASS = 96
N_ST = 8


def draw_decay_shift(key, part):
    sequence_number = TOKEN_TOTAL // TOKENS_PER_SEQ
    span_count = TOKENS_PER_SEQ // MBLOCK
    base_key, spot_key, random_size_key = jax.random.split(key, 3)
    shift_baseline = jax.random.uniform(base_key, (sequence_number, span_count, 1, 1), jnp.float32, -0.8, 0.8)
    shift_baseline = jnp.broadcast_to(shift_baseline, (sequence_number, span_count, MBLOCK, MIXER_HEADS))
    shift_baseline = shift_baseline.reshape(sequence_number, TOKENS_PER_SEQ, MIXER_HEADS)
    spot_pos = jax.random.randint(spot_key, (sequence_number, 3, MIXER_HEADS), 0, TOKENS_PER_SEQ)
    target_location = jnp.arange(TOKENS_PER_SEQ)[None, :, None, None] == spot_pos[:, None, :, :]
    spike_addition = jnp.any(target_location, axis=2).astype(jnp.float32)
    spike_addition = spike_addition * jax.random.uniform(random_size_key, (sequence_number, TOKENS_PER_SEQ, MIXER_HEADS), jnp.float32, 7.0, 9.0)
    return (shift_baseline + spike_addition).reshape(TOKEN_TOTAL, MIXER_HEADS)


def draw_passage_ids(key, part):
    blk_dev = TOKENS_PER_SEQ // QBLOCK
    slot_count = blk_dev * PER_BLOCK
    capacity = max(2, -(-slot_count // N_ST))
    positions = N_ST * capacity

    def one_sequence(seq_key, seq_index):
        keys_five = jax.random.split(seq_key, 5)
        place = jnp.arange(positions)
        offset = place // capacity
        copy_idx = place % capacity
        forced = (offset == N_ST - 1) | (offset == N_ST // 2) & (copy_idx == 0)
        score = jax.random.randint(keys_five[0], (positions,), 0, 1 << 20)
        score = jnp.where(forced, -1, score) * positions + place
        chosen = jnp.argsort(score)[:slot_count]
        owner_of = (seq_index + offset[chosen]) % N_ST
        mixing = jax.random.randint(keys_five[1], (slot_count,), 0, 1 << 20) * slot_count + jnp.arange(slot_count)
        owner_of = owner_of[jnp.argsort(mixing)]
        local_idx = jax.random.randint(keys_five[2], (slot_count,), 0, PASS_DEV)
        local_idx = jnp.minimum(local_idx, jax.random.randint(keys_five[3], (slot_count,), 0, PASS_DEV))
        local_idx = jnp.minimum(local_idx, jax.random.randint(keys_five[4], (slot_count,), 0, PASS_DEV))
        return (owner_of * PASS_DEV + local_idx).reshape(blk_dev, PER_BLOCK)
    seq_keys = jax.random.split(jax.random.fold_in(key, 11), N_ST)
    picked = jax.vmap(one_sequence)(seq_keys, jnp.arange(N_ST))
    return picked.reshape(N_ST * blk_dev, PER_BLOCK).astype(jnp.int32)


def block_levels(own_key, shape, shards, least, high):
    factor_of = 1.0
    for dim, blocks in shards:
        heights = jax.random.uniform(jax.random.fold_in(jax.random.fold_in(own_key, 6), dim), (blocks,), jnp.float32, least / len(shards), high / len(shards))
        factor_of = factor_of * jnp.repeat(jnp.exp(heights), shape[dim] // blocks).reshape((-1,) + (1,) * (len(shape) - 1 - dim))
    return factor_of


def noise(own_key, shape, width, bound, cuts=(), dtype=jnp.bfloat16):
    level = block_levels(own_key, shape, cuts, -0.22, 0.18) if cuts else 1.0
    entries = jax.random.normal(own_key, shape, jnp.float32) * width * level
    return jnp.minimum(jnp.maximum(entries, -bound), bound).astype(dtype)


def setup_inputs(seed: int = 0) -> dict:
    keys = jax.random.split(jax.random.key(seed), 22)
    tokens = noise(keys[0], (TOKEN_TOTAL, MODEL_DIM), 1.0, 6.0, ((0, 8),))
    mix_query = noise(keys[1], (MODEL_DIM, MIXER_WIDTH), MODEL_DIM ** -0.5, 0.125, ((1, 4),))
    mix_key = noise(keys[2], (MODEL_DIM, MIXER_WIDTH), MODEL_DIM ** -0.5, 0.125, ((1, 4),))
    mix_value = noise(keys[3], (MODEL_DIM, MIXER_WIDTH), MODEL_DIM ** -0.5, 0.125, ((1, 4),))
    decay_lower_map = noise(keys[4], (MODEL_DIM, LOWRANK_WIDTH), MODEL_DIM ** -0.5, 0.125)
    decay_upper_map = noise(keys[5], (LOWRANK_WIDTH, MIXER_WIDTH), (LOWRANK_WIDTH // 2) ** -0.5, 1.0, ((1, 4),))
    decay_base = jnp.clip(-7.5 + 5.0 * jax.random.uniform(keys[6], (MIXER_WIDTH,), jnp.float32) ** block_levels(keys[6], (MIXER_WIDTH,), ((0, 4),), -0.2, 0.2), -7.5, -2.5)
    decay_shift = draw_decay_shift(jax.random.fold_in(keys[21], 71), 0)
    rate_lower_map = noise(keys[8], (MODEL_DIM, LOWRANK_WIDTH), MODEL_DIM ** -0.5, 0.125)
    rate_upper_map = noise(keys[9], (LOWRANK_WIDTH, MIXER_WIDTH), LOWRANK_WIDTH ** -0.5, 0.75, ((1, 4),))
    norm_gain = jnp.clip(1.0 + 0.18 * jax.random.normal(keys[10], (MIXER_WIDTH,), jnp.float32), 0.1, 1.9)
    mix_out = noise(keys[11], (MIXER_WIDTH, MODEL_DIM), MIXER_WIDTH ** -0.5, 0.1875, ((1, 4),))
    cross_query = noise(keys[12], (MODEL_DIM, XWIDTH), MODEL_DIM ** -0.5, 0.125, ((1, 4),))
    score_gain = jnp.clip(1.0 + 0.18 * jax.random.normal(keys[13], (XWIDTH,), jnp.float32), 0.1, 1.9)
    passage_key = noise(keys[14], (MODEL_DIM, XWIDTH), MODEL_DIM ** -0.5, 0.125, ((1, 4),))
    passage_value = noise(keys[15], (MODEL_DIM, XWIDTH), MODEL_DIM ** -0.5, 0.125, ((1, 4),))
    cross_out = noise(keys[16], (XWIDTH, MODEL_DIM), (XWIDTH // 16) ** -0.5, 0.5, ((1, 4),))
    gate_down = noise(keys[17], (MODEL_DIM, GLORA), MODEL_DIM ** -0.5, 0.125)
    gate_up = noise(keys[18], (GLORA, MODEL_DIM), GLORA ** -0.5, 0.5, ((1, 4),))
    store = noise(keys[19], (NPASS, PLEN, MODEL_DIM), 1.0, 6.0, ((0, 8),))
    passage_ids = draw_passage_ids(jax.random.fold_in(keys[21], 71), 0)
    return dict(tokens=tokens, mix_query=mix_query, mix_key=mix_key, mix_value=mix_value, decay_lower_map=decay_lower_map, decay_upper_map=decay_upper_map, decay_base=decay_base, decay_shift=decay_shift, rate_lower_map=rate_lower_map, rate_upper_map=rate_upper_map, norm_gain=norm_gain, mix_out=mix_out, cross_query=cross_query, score_gain=score_gain, passage_key=passage_key, passage_value=passage_value, cross_out=cross_out, gate_down=gate_down, gate_up=gate_up, store=store, passage_ids=passage_ids)


FLOAT32 = jnp.float32
BFLOAT = jnp.bfloat16
PRECISE = lax.Precision.HIGHEST

def rounded(values):
    return lax.optimization_barrier(values.astype(BFLOAT)).astype(FLOAT32)

def head_norm(values, head_size):
    shaped = values.reshape(values.shape[:-1] + (values.shape[-1] // head_size, head_size))
    scaled = shaped * lax.rsqrt(lax.optimization_barrier(jnp.mean(shaped * shaped, axis=-1, keepdims=True)) + 1e-06)
    return scaled.reshape(values.shape)

def recurrent_step(state, inputs):
    query_vec, fade_t, key_vec, value_vec, unit_key, rate_gate = inputs
    pulled = jnp.einsum('bhij,bhj->bhi', state, -unit_key, precision=PRECISE)
    state = state * fade_t[:, :, None, :] + pulled[..., :, None] * (unit_key * rate_gate)[..., None, :] + value_vec[..., :, None] * key_vec[..., None, :]
    return (state, jnp.einsum('bhij,bhj->bhi', state, query_vec, precision=PRECISE))

def reference(tokens, mix_query, mix_key, mix_value, decay_lower_map, decay_upper_map, decay_base, decay_shift, rate_lower_map, rate_upper_map, norm_gain, mix_out, cross_query, score_gain, passage_key, passage_value, cross_out, gate_down, gate_up, store, passage_ids):
    total_rows = tokens.shape[0]
    sequence_number = total_rows // TOKENS_PER_SEQ

    def project(weight):
        return rounded(jnp.dot(tokens, weight, preferred_element_type=FLOAT32))
    query_vec = project(mix_query)
    key_vec = project(mix_key)
    value_vec = project(mix_value)
    decay_low = jnp.tanh(jnp.dot(tokens, decay_lower_map, preferred_element_type=FLOAT32)).astype(BFLOAT)
    decay_pre = decay_base + jnp.dot(decay_low, decay_upper_map, preferred_element_type=FLOAT32) + jnp.repeat(decay_shift, RHEAD, axis=1)
    log_fade = -jnp.exp(-jax.nn.softplus(-decay_pre) - 0.5)
    rate_low = jnp.dot(tokens, rate_lower_map, preferred_element_type=FLOAT32).astype(BFLOAT)
    rate_gate = jax.nn.sigmoid(jnp.dot(rate_low, rate_upper_map, preferred_element_type=FLOAT32))

    def by_time(values):
        return jnp.moveaxis(values.reshape(sequence_number, TOKENS_PER_SEQ, MIXER_HEADS, RHEAD), 1, 0)
    keyed = key_vec.reshape(total_rows, MIXER_HEADS, RHEAD)
    unit_key = keyed * lax.rsqrt(lax.optimization_barrier(jnp.sum(keyed * keyed, axis=-1, keepdims=True)) + 1e-06)
    sequence_in = (by_time(query_vec), by_time(jnp.exp(log_fade)), by_time(key_vec), by_time(value_vec), by_time(unit_key), by_time(rate_gate))
    state_zero = jnp.zeros((sequence_number, MIXER_HEADS, RHEAD, RHEAD), FLOAT32)
    _, head_out = lax.scan(recurrent_step, state_zero, sequence_in)
    head_out = jnp.moveaxis(head_out, 0, 1).reshape(total_rows, MIXER_HEADS, RHEAD)
    centred = head_out - lax.optimization_barrier(jnp.mean(head_out, axis=-1, keepdims=True))
    spread = lax.optimization_barrier(jnp.mean(centred * centred, axis=-1, keepdims=True))
    mixer_heads = (centred * lax.rsqrt(spread + 0.00064)).reshape(total_rows, MIXER_WIDTH)
    mixer_heads = (mixer_heads * norm_gain).astype(BFLOAT)
    queries = head_norm(jnp.dot(tokens, cross_query, preferred_element_type=FLOAT32), XHEAD) * score_gain
    queries = queries.astype(BFLOAT)
    store_rows = store.reshape(-1, MODEL_DIM)
    keys_all = head_norm(jnp.dot(store_rows, passage_key, preferred_element_type=FLOAT32), XHEAD)
    keys_all = keys_all.astype(BFLOAT).reshape(-1, PLEN, XWIDTH)
    values_all = jnp.dot(store_rows, passage_value, preferred_element_type=FLOAT32).astype(BFLOAT)
    values_all = values_all.reshape(-1, PLEN, XWIDTH)

    def attend(item):
        block_q, block_ids = item
        block_keys = keys_all[block_ids].reshape(-1, XHEADS, XHEAD).astype(FLOAT32)
        block_values = values_all[block_ids].reshape(-1, XHEADS, XHEAD).astype(FLOAT32)
        block_q = block_q.reshape(QBLOCK, XHEADS, XHEAD).astype(FLOAT32)
        scores = jnp.einsum('qhd,khd->hqk', block_q, block_keys, precision=PRECISE) * XHEAD ** (-0.5)
        expon = jnp.exp(scores)
        weights = rounded(expon / lax.optimization_barrier(jnp.sum(expon, axis=-1, keepdims=True)))
        result = jnp.einsum('hqk,khd->qhd', weights, block_values, precision=PRECISE)
        return result.astype(BFLOAT).reshape(QBLOCK, XWIDTH)
    attended = lax.map(attend, (queries.reshape(-1, QBLOCK, XWIDTH), passage_ids)).reshape(total_rows, XWIDTH)
    gate_low = jnp.dot(tokens, gate_down, preferred_element_type=FLOAT32).astype(BFLOAT)
    gate_open = jax.nn.sigmoid(jnp.dot(gate_low, gate_up, preferred_element_type=FLOAT32))
    mixer_part = jnp.dot(mixer_heads, mix_out, preferred_element_type=FLOAT32)
    cross_part = jnp.dot(attended, cross_out, preferred_element_type=FLOAT32)
    return (mixer_part + gate_open * cross_part).astype(BFLOAT)
```

```python
import functools
import jax
import jax.numpy as jnp
from jax import lax
from jax.experimental import pallas as pl
from jax.experimental.pallas import tpu as pltpu
from jax.sharding import PartitionSpec as P

XHEAD = 256
QBLOCK = 64
MBLOCK = 64
RHEAD = 64
LROWS = 16

FLOAT32 = jnp.float32
BFLOAT = jnp.bfloat16
PRECISE = lax.Precision.HIGHEST
VMEM = pltpu.VMEM
SMEM = pltpu.SMEM
NT = (((1,), (1,)), ((), ()))
NN = (((1,), (0,)), ((), ()))
TN = (((0,), (0,)), ((), ()))


def dot(left, right, dims=NN, precision=None):
    return lax.dot_general(left, right, dims, precision=precision, preferred_element_type=FLOAT32)


def iota(shape, dim):
    return lax.broadcasted_iota(jnp.int32, shape, dim)


def whole(count):
    return [pl.BlockSpec(memory_space=VMEM)] * count


def table_kernel(pass_dev, per_block, ids_ref, want_ref, blk_ref, own_ref, rank_ref, fill_ref):
    owners, capacity = want_ref.shape
    slots = ids_ref.shape[0] * ids_ref.shape[1]

    def clear(o, carry):
        fill_ref[o] = 0
        for r in range(capacity):
            want_ref[o, r] = 0
            blk_ref[o, r] = 0
        return carry

    lax.fori_loop(0, owners, clear, 0)

    def put(n, carry):
        passage = ids_ref[n // per_block, n % per_block]
        owner = passage // pass_dev
        rank = fill_ref[owner]
        fill_ref[owner] = rank + 1
        own_ref[n] = owner
        rank_ref[n] = rank
        want_ref[owner, rank] = passage - owner * pass_dev
        blk_ref[owner, rank] = n // per_block
        return carry

    lax.fori_loop(0, slots, put, 0)


def make_tables(passage_ids, owners, capacity, pass_dev):
    slots = passage_ids.shape[0] * passage_ids.shape[1]
    smem = pl.BlockSpec(memory_space=SMEM)
    return pl.pallas_call(
        functools.partial(table_kernel, pass_dev, passage_ids.shape[1]),
        out_shape=[
            jax.ShapeDtypeStruct((owners, capacity), jnp.int32),
            jax.ShapeDtypeStruct((owners, capacity), jnp.int32),
            jax.ShapeDtypeStruct((slots,), jnp.int32),
            jax.ShapeDtypeStruct((slots,), jnp.int32),
        ],
        in_specs=[smem],
        out_specs=[smem] * 4,
        scratch_shapes=[SMEM((owners,), jnp.int32)],
        name="tables",
    )(passage_ids)


def query_kernel(blk_ref, tok_ref, w_ref, gain_ref, out_ref, q_ref):
    width = w_ref.shape[1]
    for h in range(width // XHEAD):
        cols = slice(h * XHEAD, (h + 1) * XHEAD)
        raw = dot(tok_ref[...], w_ref[:, cols])
        scale = lax.rsqrt(jnp.mean(raw * raw, axis=-1, keepdims=True) + 1e-06)
        q_ref[:, cols] = (raw * scale * gain_ref[:, cols]).astype(BFLOAT)
    owners, capacity = blk_ref.shape

    def copy(o, carry):
        for r in range(capacity):
            start = pl.multiple_of(blk_ref[o, r] * QBLOCK, QBLOCK)
            out_ref[o, r * QBLOCK : (r + 1) * QBLOCK, :] = q_ref[pl.ds(start, QBLOCK), :]
        return carry

    lax.fori_loop(0, owners, copy, 0)


def make_queries(blk, tokens, cross_query, score_gain):
    owners, capacity = blk.shape
    width = cross_query.shape[1]
    return pl.pallas_call(
        query_kernel,
        out_shape=jax.ShapeDtypeStruct((owners, capacity * QBLOCK, width), BFLOAT),
        in_specs=[pl.BlockSpec(memory_space=SMEM)] + whole(3),
        out_specs=pl.BlockSpec(memory_space=VMEM),
        scratch_shapes=[VMEM((tokens.shape[0], width), BFLOAT)],
        name="queries",
    )(blk, tokens, cross_query, score_gain.reshape(1, -1))


def keyval_kernel(rows_ref, wk_ref, wv_ref, k_ref, v_ref):
    width = wk_ref.shape[1]
    rows = rows_ref[...]
    for h in range(width // XHEAD):
        cols = slice(h * XHEAD, (h + 1) * XHEAD)
        raw = dot(rows, wk_ref[:, cols])
        scale = lax.rsqrt(jnp.mean(raw * raw, axis=-1, keepdims=True) + 1e-06)
        k_ref[:, cols] = (raw * scale).astype(BFLOAT)
        v_ref[:, cols] = dot(rows, wv_ref[:, cols]).astype(BFLOAT)


def make_keyvals(store, passage_key, passage_value):
    pass_dev, plen, model = store.shape
    width = passage_key.shape[1]
    group = max(g for g in range(1, 5) if pass_dev % g == 0)
    tile = group * plen
    weight = pl.BlockSpec((model, width), lambda i: (0, 0))
    out = pl.BlockSpec((tile, width), lambda i: (i, 0))
    shape = jax.ShapeDtypeStruct((pass_dev * plen, width), BFLOAT)
    return pl.pallas_call(
        keyval_kernel,
        grid=(pass_dev // group,),
        out_shape=[shape, shape],
        in_specs=[pl.BlockSpec((tile, model), lambda i: (i, 0)), weight, weight],
        out_specs=[out, out],
        name="keyvals",
    )(store.reshape(-1, model), passage_key, passage_value)


def project_kernel(
    tok_ref, mq_ref, mk_ref, mv_ref, dl_ref, rl_ref, gd_ref, du_ref, ru_ref, gu_ref,
    base_ref, shift_ref,
    q_ref, k_ref, v_ref, u_ref, rk_ref, lf_ref, gate_ref,
):
    tokens = tok_ref[...]
    width = mq_ref.shape[1]
    rank = dl_ref.shape[1]
    lows = dot(tokens, jnp.concatenate([dl_ref[...], rl_ref[...], gd_ref[...]], axis=1))
    decay_low = jnp.tanh(lows[:, :rank]).astype(BFLOAT)
    rate_low = lows[:, rank : 2 * rank].astype(BFLOAT)
    gate_low = lows[:, 2 * rank :].astype(BFLOAT)
    gate_ref[...] = jax.nn.sigmoid(dot(gate_low, gu_ref[...]))
    pre = base_ref[...] + dot(decay_low, du_ref[...])
    head = iota(pre.shape, 1) // RHEAD
    shift = jnp.zeros_like(pre)
    for h in range(width // RHEAD):
        shift = jnp.where(head == h, shift_ref[:, h : h + 1], shift)
    lf_ref[...] = -jax.nn.sigmoid(pre + shift) * (2.718281828459045 ** -0.5)
    q_ref[...] = dot(tokens, mq_ref[...]).astype(BFLOAT)
    v_ref[...] = dot(tokens, mv_ref[...]).astype(BFLOAT)
    key = dot(tokens, mk_ref[...]).astype(BFLOAT)
    k_ref[...] = key
    key = key.astype(FLOAT32)
    same = (iota((width, width), 0) // RHEAD == iota((width, width), 1) // RHEAD).astype(FLOAT32)
    unit = key * lax.rsqrt(dot(key * key, same, precision=PRECISE) + 1e-06)
    u_ref[...] = unit
    rk_ref[...] = unit * jax.nn.sigmoid(dot(rate_low, ru_ref[...]))


def project(tokens, mix_query, mix_key, mix_value, decay_lower, decay_upper, decay_base,
            decay_shift, rate_lower, rate_upper, gate_down, gate_up):
    rows = tokens.shape[0]
    width = mix_query.shape[1]
    half = jax.ShapeDtypeStruct((rows, width), BFLOAT)
    full = jax.ShapeDtypeStruct((rows, width), FLOAT32)
    return pl.pallas_call(
        project_kernel,
        out_shape=[half, half, half, full, full, full,
                   jax.ShapeDtypeStruct((rows, gate_up.shape[1]), FLOAT32)],
        in_specs=whole(12),
        out_specs=whole(7),
        name="project",
    )(tokens, mix_query, mix_key, mix_value, decay_lower, rate_lower, gate_down,
      decay_upper, rate_upper, gate_up, decay_base.reshape(1, -1), decay_shift)


def spread(value):
    rows, width = value.shape
    heads = width // RHEAD
    tiled = jnp.concatenate([value] * heads, axis=0)
    keep = iota(tiled.shape, 0) // rows == iota(tiled.shape, 1) // RHEAD
    return jnp.where(keep, tiled, jnp.zeros_like(tiled))


def fold(value):
    width = value.shape[1]
    keep = iota(value.shape, 0) // RHEAD == iota(value.shape, 1) // RHEAD
    kept = jnp.where(keep, value, jnp.zeros_like(value))
    total = kept[:RHEAD]
    for h in range(1, width // RHEAD):
        total = total + kept[h * RHEAD : (h + 1) * RHEAD]
    return total


def prepare_chunk(query, key, value, unit, rate_key, log_fade):
    length, width = query.shape
    mm = functools.partial(dot, precision=PRECISE)
    lower = (iota((length, length), 1) <= iota((length, length), 0)).astype(FLOAT32)
    cumul = mm(lower, log_fade)
    before = cumul - log_fade
    end = cumul[length - 1 :, :]
    grown = jnp.exp(-cumul)
    pulled = -unit * jnp.exp(before)
    read = query * jnp.exp(cumul)
    both = jnp.concatenate([pulled, read], axis=0)
    row = iota((length, width), 0)
    col = iota((length, width), 1) % RHEAD
    from_key = mm(both, spread(key * grown), NT)
    from_rate = mm(both, spread(rate_key * grown), NT)
    key_pull = jnp.where(col < row, from_key[:length], 0.0)
    rate_pull = jnp.where(col < row, from_rate[:length], 0.0)
    key_read = jnp.where(col <= row, from_key[length:], 0.0)
    rate_read = jnp.where(col <= row, from_rate[length:], 0.0)

    def pick(size):
        keep = (row // (2 * size) == col // (2 * size)) & ((row // size) % 2 == 1)
        return jnp.where(keep & ((col // size) % 2 == 0), rate_pull, 0.0)

    inverse = (row == col).astype(FLOAT32) + pick(1)
    size = 2
    while size < length:
        inverse = inverse + mm(mm(inverse, spread(pick(size))), spread(inverse))
        size *= 2
    wide_value = spread(value)
    moved = mm(inverse, spread(pulled))
    base = mm(inverse, spread(mm(key_pull, wide_value)))
    query_end = read + mm(rate_read, spread(moved))
    out_base = mm(key_read, wide_value) + mm(rate_read, spread(base))
    left = jnp.exp(end - cumul)
    key_left = key * left
    rate_left = rate_key * left
    fade = (iota((RHEAD, width), 0) == iota((RHEAD, width), 1) % RHEAD).astype(FLOAT32) * jnp.exp(end)
    step = fade + fold(mm(moved, rate_left, TN))
    add = fold(mm(value, key_left, TN) + mm(base, rate_left, TN))
    return query_end, out_base, step, add


def prepare_kernel(q_ref, k_ref, v_ref, u_ref, rk_ref, lf_ref, qe_ref, ob_ref, st_ref, ad_ref):
    for c in range(q_ref.shape[0] // MBLOCK):
        rows = slice(c * MBLOCK, (c + 1) * MBLOCK)
        outs = prepare_chunk(
            q_ref[rows].astype(FLOAT32), k_ref[rows].astype(FLOAT32), v_ref[rows].astype(FLOAT32),
            u_ref[rows], rk_ref[rows], lf_ref[rows])
        for ref, out in zip((qe_ref, ob_ref, st_ref, ad_ref), outs):
            ref[rows] = out


def prepare(query, key, value, unit, rate_key, log_fade):
    rows, width = query.shape
    tile = 2 * MBLOCK
    spec = pl.BlockSpec((tile, width), lambda i: (i, 0))
    full = jax.ShapeDtypeStruct((rows, width), FLOAT32)
    return pl.pallas_call(
        prepare_kernel,
        grid=(rows // tile,),
        out_shape=[full] * 4,
        in_specs=[spec] * 6,
        out_specs=[spec] * 4,
        name="prepare",
    )(query, key, value, unit, rate_key, log_fade)


def scan_kernel(qe_ref, ob_ref, st_ref, ad_ref, gain_ref, out_ref, state_ref):
    width = qe_ref.shape[1]
    mm = functools.partial(dot, precision=PRECISE)
    mean_of = (iota((width, width), 0) // RHEAD == iota((width, width), 1) // RHEAD).astype(FLOAT32)
    state_ref[...] = jnp.zeros_like(state_ref)

    def step(c, carry):
        rows = pl.ds(pl.multiple_of(c * MBLOCK, MBLOCK), MBLOCK)
        state = state_ref[...]
        out = mm(qe_ref[rows, :], spread(state), NT) + ob_ref[rows, :]
        state_ref[...] = mm(state, spread(st_ref[rows, :])) + ad_ref[rows, :]
        centred = out - mm(out, mean_of) * (1.0 / RHEAD)
        var = mm(centred * centred, mean_of) * (1.0 / RHEAD)
        out_ref[rows, :] = (centred * lax.rsqrt(var + 0.00064) * gain_ref[...]).astype(BFLOAT)
        return carry

    lax.fori_loop(0, qe_ref.shape[0] // MBLOCK, step, 0)


def scan(query_end, out_base, step, add, norm_gain):
    rows, width = query_end.shape
    return pl.pallas_call(
        scan_kernel,
        out_shape=jax.ShapeDtypeStruct((rows, width), BFLOAT),
        in_specs=whole(5),
        out_specs=pl.BlockSpec(memory_space=VMEM),
        scratch_shapes=[VMEM((RHEAD, width), FLOAT32)],
        name="scan",
    )(query_end, out_base, step, add, norm_gain.reshape(1, -1))


def attend_kernel(plen, asked_ref, q_ref, k_ref, v_ref, out_ref):
    seq = pl.program_id(0)
    width = q_ref.shape[2]
    heads = width // XHEAD
    capacity = asked_ref.shape[2]
    ones = jnp.ones((8, plen), BFLOAT)
    sums = jnp.zeros((LROWS, QBLOCK), FLOAT32)
    rowid = iota((LROWS, QBLOCK), 0)
    for r in range(capacity):
        rows = pl.ds(pl.multiple_of(asked_ref[seq, 0, r] * plen, plen), plen)
        mine = slice(r * QBLOCK, (r + 1) * QBLOCK)
        for h in range(heads):
            cols = slice(h * XHEAD, (h + 1) * XHEAD)
            scores = dot(q_ref[0, mine, cols], k_ref[rows, cols], NT) * XHEAD ** (-0.5)
            expon = jnp.exp(scores).astype(BFLOAT)
            out_ref[0, mine, cols] = dot(expon, v_ref[rows, cols]).astype(BFLOAT)
            total = dot(ones, expon, NT)[:1]
            high = total.astype(BFLOAT).astype(FLOAT32)
            where = 2 * (r * heads + h)
            sums = jnp.where(rowid == where, high, sums)
            sums = jnp.where(rowid == where + 1, total - high, sums)
    out_ref[0, capacity * QBLOCK :, :] = jnp.zeros((LROWS, width), BFLOAT)
    out_ref[0, capacity * QBLOCK :, :QBLOCK] = sums.astype(BFLOAT)


def attend(asked, queries, keys, values, plen):
    owners, qrows, width = queries.shape
    everything = pl.BlockSpec(keys.shape, lambda i, a: (0, 0))
    return pl.pallas_call(
        functools.partial(attend_kernel, plen),
        grid_spec=pltpu.PrefetchScalarGridSpec(
            num_scalar_prefetch=1,
            grid=(owners,),
            in_specs=[pl.BlockSpec((1, qrows, width), lambda i, a: (i, 0, 0)), everything, everything],
            out_specs=pl.BlockSpec((1, qrows + LROWS, width), lambda i, a: (i, 0, 0)),
        ),
        out_shape=jax.ShapeDtypeStruct((owners, qrows + LROWS, width), BFLOAT),
        name="attend",
    )(asked, queries, keys, values)


def combine_kernel(per_block, own_ref, rank_ref, part_ref, out_ref):
    width = part_ref.shape[2]
    heads = width // XHEAD
    qrows = part_ref.shape[1] - LROWS
    rowid = iota((LROWS, QBLOCK), 0)
    selrow = iota((LROWS, XHEAD), 0)

    def block(b, carry):
        total = jnp.zeros((QBLOCK, width), FLOAT32)
        sums = jnp.zeros((LROWS, QBLOCK), FLOAT32)
        for i in range(per_block):
            owner = own_ref[b * per_block + i]
            rank = rank_ref[b * per_block + i]
            rows = pl.ds(pl.multiple_of(rank * QBLOCK, QBLOCK), QBLOCK)
            total = total + part_ref[owner, rows, :].astype(FLOAT32)
            lines = part_ref[owner, qrows:, :QBLOCK].astype(FLOAT32)
            sums = sums + jnp.where(rowid // (2 * heads) == rank, lines, 0.0)
        mine = pl.ds(pl.multiple_of(b * QBLOCK, QBLOCK), QBLOCK)
        for h in range(heads):
            cols = slice(h * XHEAD, (h + 1) * XHEAD)
            choose = ((selrow // 2) % heads == h).astype(FLOAT32)
            weight = dot(sums, choose, TN, precision=PRECISE)
            out_ref[mine, cols] = (total[:, cols] / weight).astype(BFLOAT)
        return carry

    lax.fori_loop(0, out_ref.shape[0] // QBLOCK, block, 0)


def combine(own, rank, parts, rows, per_block):
    smem = pl.BlockSpec(memory_space=SMEM)
    return pl.pallas_call(
        functools.partial(combine_kernel, per_block),
        out_shape=jax.ShapeDtypeStruct((rows, parts.shape[2]), BFLOAT),
        in_specs=[smem, smem] + whole(1),
        out_specs=pl.BlockSpec(memory_space=VMEM),
        name="combine",
    )(own, rank, parts)


def gathered_dot(pieces, me, w_ref):
    total = None
    for j, piece in enumerate(pieces):
        depth = piece.shape[1]
        rows = pl.ds(pl.multiple_of((me ^ j) * depth, depth), depth)
        part = dot(piece[...], w_ref[rows, :])
        total = part if total is None else total + part
    return total


def mixer_out_kernel(me_ref, *refs):
    *pieces, w_ref, out_ref = refs
    out_ref[...] = gathered_dot(pieces, me_ref[0], w_ref)


def final_kernel(me_ref, *refs):
    *pieces, w_ref, gate_ref, mixer_ref, out_ref = refs
    cross = gathered_dot(pieces, me_ref[0], w_ref)
    out_ref[...] = (mixer_ref[...] + gate_ref[...] * cross).astype(BFLOAT)


def over_tp(body, me, pieces, others, dtype, name):
    shape = (pieces[0].shape[0], others[0].shape[1])
    return pl.pallas_call(
        body,
        out_shape=jax.ShapeDtypeStruct(shape, dtype),
        in_specs=[pl.BlockSpec(memory_space=SMEM)] + whole(len(pieces) + len(others)),
        out_specs=pl.BlockSpec(memory_space=VMEM),
        name=name,
    )(me, *pieces, *others)


def gather_tp(piece, count):
    pieces = {0: piece}
    bit = count // 2
    while bit:
        pairs = [(i, i ^ bit) for i in range(count)]
        for j in list(pieces):
            pieces[j ^ bit] = lax.ppermute(pieces[j], "tp", pairs)
        bit //= 2
    return [pieces[j] for j in range(count)]


def local(
    tokens, mix_query, mix_key, mix_value, decay_lower_map, decay_upper_map, decay_base,
    decay_shift, rate_lower_map, rate_upper_map, norm_gain, mix_out, cross_query, score_gain,
    passage_key, passage_value, cross_out, gate_down, gate_up, store, passage_ids,
):
    rows = tokens.shape[0]
    owners = lax.axis_size("st")
    shards = lax.axis_size("tp")
    pass_dev, plen, _ = store.shape
    per_block = passage_ids.shape[1]
    slots = passage_ids.shape[0] * per_block
    capacity = max(2, -(-slots // owners))
    me = lax.axis_index("tp").astype(jnp.int32).reshape(1)

    want, blk, own, rank = make_tables(passage_ids, owners, capacity, pass_dev)
    asked = lax.all_to_all(want[:, None, :], "st", split_axis=0, concat_axis=0, tiled=True)
    queries = make_queries(blk, tokens, cross_query, score_gain)
    queries = lax.all_to_all(queries, "st", split_axis=0, concat_axis=0, tiled=True)
    keys, values = make_keyvals(store, passage_key, passage_value)
    *mixer_in, gate = project(
        tokens, mix_query, mix_key, mix_value, decay_lower_map, decay_upper_map, decay_base,
        decay_shift, rate_lower_map, rate_upper_map, gate_down, gate_up)
    prepared = prepare(*mixer_in)
    parts = attend(asked, queries, keys, values, plen)
    parts = lax.all_to_all(parts, "st", split_axis=0, concat_axis=0, tiled=True)
    mixer_heads = scan(*prepared, norm_gain)
    mixer_part = over_tp(mixer_out_kernel, me, gather_tp(mixer_heads, shards), [mix_out],
                         FLOAT32, "mixer_out")
    attended = combine(own, rank, parts, rows, per_block)
    return over_tp(final_kernel, me, gather_tp(attended, shards), [cross_out, gate, mixer_part],
                   BFLOAT, "final")


def solution(mesh):
    placed = (
        P("st", None), P(None, "tp"), P(None, "tp"), P(None, "tp"), P(), P(None, "tp"), P("tp"),
        P("st", "tp"), P(), P(None, "tp"), P("tp"), P(None, "tp"), P(None, "tp"), P("tp"),
        P(None, "tp"), P(None, "tp"), P(None, "tp"), P(), P(None, "tp"), P("st", None, None),
        P("st", None),
    )
    return jax.shard_map(
        local, mesh=mesh, in_specs=placed, out_specs=P("st", "tp"), check_vma=False
    )
```

```python
import functools
import jax
import jax.numpy as jnp
from jax import lax
from jax.experimental import pallas as pl
from jax.experimental.pallas import tpu as pltpu
from jax.sharding import PartitionSpec as P

XHEAD = 256
QBLOCK = 64
MBLOCK = 64
RHEAD = 64
LROWS = 16

FLOAT32 = jnp.float32
BFLOAT = jnp.bfloat16
PRECISE = lax.Precision.HIGHEST
VMEM = pltpu.VMEM
SMEM = pltpu.SMEM
NT = (((1,), (1,)), ((), ()))
NN = (((1,), (0,)), ((), ()))
TN = (((0,), (0,)), ((), ()))


def dot(left, right, dims=NN, precision=None):
    return lax.dot_general(left, right, dims, precision=precision, preferred_element_type=FLOAT32)


def iota(shape, dim):
    return lax.broadcasted_iota(jnp.int32, shape, dim)


def whole(count):
    return [pl.BlockSpec(memory_space=VMEM)] * count


def after(refs, count):
    return [pl.BlockSpec(memory_space=pl.ANY)] * count


def up16(count):
    return -(-count // 16) * 16


def entry(lines, row, lane):
    hit = (iota(lines.shape, 0) == row) & (iota(lines.shape, 1) == lane)
    return jnp.sum(jnp.where(hit, lines, 0.0)).astype(jnp.int32)


def write_group(out_ref, q_ref, blocks, passages):
    capacity = len(blocks)
    width = out_ref.shape[1]
    line = jnp.zeros((LROWS, width), FLOAT32)
    row, lane = iota(line.shape, 0), iota(line.shape, 1)
    for r in range(capacity):
        start = pl.multiple_of(jnp.maximum(blocks[r] - 1, 0) * QBLOCK, QBLOCK)
        out_ref[r * QBLOCK : (r + 1) * QBLOCK, :] = q_ref[pl.ds(start, QBLOCK), :]
        line = jnp.where((row == 0) & (lane == r), passages[r].astype(FLOAT32), line)
    out_ref[capacity * QBLOCK :, :] = line.astype(BFLOAT)


def query_kernel(pass_dev, owners, me_ref, ids_ref, tok_ref, w_ref, gain_ref, q_ref, blk_ref,
                 *refs):
    *group_refs, pidx_ref, fill_ref = refs
    capacity = blk_ref.shape[1]
    per_block = ids_ref.shape[1]
    rows = tok_ref.shape[0]
    width = w_ref.shape[1]

    def clear(o, carry):
        fill_ref[o] = 0
        for r in range(capacity):
            pidx_ref[o, r] = 0
            blk_ref[o, r] = 0
        return carry

    lax.fori_loop(0, owners, clear, 0)

    def put(n, carry):
        passage = ids_ref[n // per_block, n % per_block]
        owner = passage // pass_dev
        rank = fill_ref[owner]
        fill_ref[owner] = rank + 1
        pidx_ref[owner, rank] = passage - owner * pass_dev
        blk_ref[owner, rank] = n // per_block + 1
        return carry

    lax.fori_loop(0, ids_ref.shape[0] * per_block, put, 0)

    for h in range(width // XHEAD):
        cols = slice(h * XHEAD, (h + 1) * XHEAD)
        raw = dot(tok_ref[...], w_ref[:, cols])
        scale = lax.rsqrt(jnp.mean(raw * raw, axis=-1, keepdims=True) + 1e-06)
        q_ref[:rows, cols] = (raw * scale * gain_ref[:, cols]).astype(BFLOAT)

    tail = q_ref.shape[0] - rows
    row, lane = iota((tail, 128), 0), iota((tail, 128), 1)

    def line(o, table):
        for r in range(capacity):
            table = jnp.where((row == o) & (lane == r), blk_ref[o, r].astype(FLOAT32), table)
            table = jnp.where((row == o) & (lane == capacity + r),
                              pidx_ref[o, r].astype(FLOAT32), table)
        return table

    table = lax.fori_loop(0, owners, line, jnp.zeros((tail, 128), FLOAT32))
    q_ref[rows:, :] = jnp.zeros((tail, width), BFLOAT)
    q_ref[rows:, :128] = table.astype(BFLOAT)
    for k, ref in enumerate(group_refs):
        owner = me_ref[0] ^ k
        write_group(ref, q_ref, [blk_ref[owner, r] for r in range(capacity)],
                    [pidx_ref[owner, r] for r in range(capacity)])


def make_queries(me, ids, owners, capacity, pass_dev, tokens, cross_query, score_gain):
    rows, width = tokens.shape[0], cross_query.shape[1]
    smem = pl.BlockSpec(memory_space=SMEM)
    group = jax.ShapeDtypeStruct((capacity * QBLOCK + LROWS, width), BFLOAT)
    count = owners // 2
    outs = pl.pallas_call(
        functools.partial(query_kernel, pass_dev, owners),
        out_shape=[jax.ShapeDtypeStruct((rows + up16(owners), width), BFLOAT),
                   jax.ShapeDtypeStruct((owners, capacity), jnp.int32)] + [group] * count,
        in_specs=[smem, smem] + whole(3),
        out_specs=whole(1) + [smem] + whole(count),
        scratch_shapes=[SMEM((owners, capacity), jnp.int32), SMEM((owners,), jnp.int32)],
        name="queries",
    )(me, ids, tokens, cross_query, score_gain.reshape(1, -1))
    return outs[0], outs[1], outs[2:]


def relay_kernel(rows, deps, me_ref, q_ref, *refs):
    blk_ref, *group_refs = refs[deps:]
    owners, capacity = blk_ref.shape
    table = q_ref[rows:, :128].astype(FLOAT32)
    for k, ref in enumerate(group_refs):
        owner = me_ref[0] ^ k
        blocks = [entry(table, owner, r) for r in range(capacity)]
        for r in range(capacity):
            blk_ref[owner, r] = blocks[r]
        write_group(ref, q_ref, blocks, [entry(table, owner, capacity + r) for r in range(capacity)])


def relay(me, queries, rows, owners, capacity, deps):
    width = queries.shape[1]
    smem = pl.BlockSpec(memory_space=SMEM)
    group = jax.ShapeDtypeStruct((capacity * QBLOCK + LROWS, width), BFLOAT)
    count = owners // 2
    outs = pl.pallas_call(
        functools.partial(relay_kernel, rows, len(deps)),
        out_shape=[jax.ShapeDtypeStruct((owners, capacity), jnp.int32)] + [group] * count,
        in_specs=[smem] + whole(1) + after(deps, len(deps)),
        out_specs=[smem] + whole(count),
        name="relay",
    )(me, queries, *deps)
    return outs[0], outs[1:]


def keyval_kernel(rows_ref, wk_ref, wv_ref, k_ref, v_ref):
    width = wk_ref.shape[1]
    rows = rows_ref[...]
    for h in range(width // XHEAD):
        cols = slice(h * XHEAD, (h + 1) * XHEAD)
        raw = dot(rows, wk_ref[:, cols])
        scale = lax.rsqrt(jnp.mean(raw * raw, axis=-1, keepdims=True) + 1e-06)
        k_ref[:, cols] = (raw * scale).astype(BFLOAT)
        v_ref[:, cols] = dot(rows, wv_ref[:, cols]).astype(BFLOAT)


def make_keyvals(store, passage_key, passage_value):
    pass_dev, plen, model = store.shape
    width = passage_key.shape[1]
    group = max(g for g in range(1, 5) if pass_dev % g == 0)
    tile = group * plen
    weight = pl.BlockSpec((model, width), lambda i: (0, 0))
    out = pl.BlockSpec((tile, width), lambda i: (i, 0))
    shape = jax.ShapeDtypeStruct((pass_dev * plen, width), BFLOAT)
    return pl.pallas_call(
        keyval_kernel,
        grid=(pass_dev // group,),
        out_shape=[shape, shape],
        in_specs=[pl.BlockSpec((tile, model), lambda i: (i, 0)), weight, weight],
        out_specs=[out, out],
        name="keyvals",
    )(store.reshape(-1, model), passage_key, passage_value)


def project_kernel(
    tok_ref, mq_ref, mk_ref, mv_ref, dl_ref, rl_ref, gd_ref, du_ref, ru_ref, gu_ref,
    base_ref, shift_ref,
    q_ref, k_ref, v_ref, u_ref, rk_ref, lf_ref, gate_ref,
):
    tokens = tok_ref[...]
    width = mq_ref.shape[1]
    rank = dl_ref.shape[1]
    lows = dot(tokens, jnp.concatenate([dl_ref[...], rl_ref[...], gd_ref[...]], axis=1))
    decay_low = jnp.tanh(lows[:, :rank]).astype(BFLOAT)
    rate_low = lows[:, rank : 2 * rank].astype(BFLOAT)
    gate_low = lows[:, 2 * rank :].astype(BFLOAT)
    gate_ref[...] = jax.nn.sigmoid(dot(gate_low, gu_ref[...]))
    pre = base_ref[...] + dot(decay_low, du_ref[...])
    head = iota(pre.shape, 1) // RHEAD
    shift = jnp.zeros_like(pre)
    for h in range(width // RHEAD):
        shift = jnp.where(head == h, shift_ref[:, h : h + 1], shift)
    lf_ref[...] = -jax.nn.sigmoid(pre + shift) * (2.718281828459045 ** -0.5)
    q_ref[...] = dot(tokens, mq_ref[...]).astype(BFLOAT)
    v_ref[...] = dot(tokens, mv_ref[...]).astype(BFLOAT)
    key = dot(tokens, mk_ref[...]).astype(BFLOAT)
    k_ref[...] = key
    key = key.astype(FLOAT32)
    same = (iota((width, width), 0) // RHEAD == iota((width, width), 1) // RHEAD).astype(FLOAT32)
    unit = key * lax.rsqrt(dot(key * key, same, precision=PRECISE) + 1e-06)
    u_ref[...] = unit
    rk_ref[...] = unit * jax.nn.sigmoid(dot(rate_low, ru_ref[...]))


def project(tokens, mix_query, mix_key, mix_value, decay_lower, decay_upper, decay_base,
            decay_shift, rate_lower, rate_upper, gate_down, gate_up):
    rows = tokens.shape[0]
    width = mix_query.shape[1]
    half = jax.ShapeDtypeStruct((rows, width), BFLOAT)
    full = jax.ShapeDtypeStruct((rows, width), FLOAT32)
    return pl.pallas_call(
        project_kernel,
        out_shape=[half, half, half, full, full, full,
                   jax.ShapeDtypeStruct((rows, gate_up.shape[1]), FLOAT32)],
        in_specs=whole(12),
        out_specs=whole(7),
        name="project",
    )(tokens, mix_query, mix_key, mix_value, decay_lower, rate_lower, gate_down,
      decay_upper, rate_upper, gate_up, decay_base.reshape(1, -1), decay_shift)


def parts2(value):
    high = value.astype(BFLOAT)
    return high, (value - high.astype(FLOAT32)).astype(BFLOAT)


def parts3(value):
    high = value.astype(BFLOAT)
    rest = value - high.astype(FLOAT32)
    return (high,) + parts2(rest)


def spread(value):
    rows, width = value.shape
    lane = iota((1, 128), 1) // RHEAD
    blank = jnp.zeros((rows, 128), value.dtype)
    blocks = []
    for h in range(width // RHEAD):
        mine = (h * RHEAD) // 128
        keep = (lane == h % (128 // RHEAD)).astype(value.dtype)
        cells = [blank] * (width // 128)
        cells[mine] = value[:, mine * 128 : (mine + 1) * 128] * keep
        blocks.append(jnp.concatenate(cells, axis=1) if len(cells) > 1 else cells[0])
    return jnp.concatenate(blocks, axis=0)


def fold(value):
    width = value.shape[1]
    lane = iota((1, 128), 1) // RHEAD
    cells = []
    for t in range(width // 128):
        cell = value[t * 128 : t * 128 + RHEAD, t * 128 : (t + 1) * 128]
        for p in range(1, 128 // RHEAD):
            start = t * 128 + p * RHEAD
            cell = jnp.where(lane == p, value[start : start + RHEAD, t * 128 : (t + 1) * 128], cell)
        cells.append(cell)
    return jnp.concatenate(cells, axis=1) if len(cells) > 1 else cells[0]


def left_of(value):
    high, low = parts2(value)
    return jnp.concatenate([high, low, high], axis=1)


def right_of(value):
    high, low = parts2(value)
    high, low = spread(high), spread(low)
    return jnp.concatenate([high, high, low], axis=0)


def right_nt(value):
    high, low = parts2(value)
    high, low = spread(high), spread(low)
    return jnp.concatenate([high, high, low], axis=1)


def across(left, right):
    lh, ll = parts2(left)
    rh, rl = parts2(right)
    return fold(dot(jnp.concatenate([lh, ll, lh], axis=0), jnp.concatenate([rh, rh, rl], axis=0), TN))


def prepare_chunks(queries, keys, values, units, rate_keys, fades):
    n = range(len(queries))
    length, width = queries[0].shape
    row = iota((length, width), 0)
    col = iota((length, width), 1) % RHEAD
    lower = (iota((length, length), 1) <= iota((length, length), 0)).astype(BFLOAT)
    cumul = []
    for c in n:
        sums = dot(lower, jnp.concatenate(parts3(fades[c]), axis=1))
        cumul.append(sums[:, :width] + sums[:, width : 2 * width] + sums[:, 2 * width :])
    ends = [cumul[c][length - 1 :, :] for c in n]
    grown = [jnp.exp(-cumul[c]) for c in n]
    pulled = [-units[c] * jnp.exp(cumul[c] - fades[c]) for c in n]
    read = [queries[c] * jnp.exp(cumul[c]) for c in n]
    both = [left_of(jnp.concatenate([pulled[c], read[c]], axis=0)) for c in n]
    from_rate = [dot(both[c], right_nt(rate_keys[c] * grown[c]), NT) for c in n]
    from_key = [dot(both[c], right_nt(keys[c] * grown[c]), NT) for c in n]
    strict, upto = col < row, col <= row
    rate_pull = [jnp.where(strict, from_rate[c][:length], 0.0) for c in n]
    rate_read = [left_of(jnp.where(upto, from_rate[c][length:], 0.0)) for c in n]
    key_both = [
        left_of(jnp.concatenate([jnp.where(strict, from_key[c][:length], 0.0),
                                 jnp.where(upto, from_key[c][length:], 0.0)], axis=0)) for c in n]

    def pick(size):
        return (row // (2 * size) == col // (2 * size)) & (row // size > col // size)

    first = pick(1)
    eye = (row == col).astype(FLOAT32)
    inverse = [eye + jnp.where(first, rate_pull[c], 0.0) for c in n]
    size = 2
    while size < length:
        keep = pick(size)
        mids = [dot(left_of(inverse[c]), right_of(jnp.where(keep, rate_pull[c], 0.0))) for c in n]
        adds = [dot(left_of(mids[c]), right_of(inverse[c])) for c in n]
        inverse = [inverse[c] + adds[c] for c in n]
        size *= 2
    inverse = [left_of(inverse[c]) for c in n]
    from_value = []
    for c in n:
        wide = spread(values[c])
        from_value.append(dot(key_both[c][:, : 2 * width], jnp.concatenate([wide, wide], axis=0)))
    moved = [dot(inverse[c], right_of(pulled[c])) for c in n]
    base = [dot(inverse[c], right_of(from_value[c][:length])) for c in n]
    query_end = [read[c] + dot(rate_read[c], right_of(moved[c])) for c in n]
    out_base = [from_value[c][length:] + dot(rate_read[c], right_of(base[c])) for c in n]
    left = [jnp.exp(ends[c] - cumul[c]) for c in n]
    step, add = [], []
    diag = iota((RHEAD, width), 0) == iota((RHEAD, width), 1) % RHEAD
    for c in n:
        rate_left = rate_keys[c] * left[c]
        step.append(jnp.where(diag, jnp.exp(ends[c]), 0.0) + across(moved[c], rate_left))
        add.append(across(jnp.concatenate([values[c].astype(FLOAT32), base[c]], axis=0),
                          jnp.concatenate([keys[c] * left[c], rate_left], axis=0)))
    return query_end, out_base, step, add


def prepare_kernel(deps, q_ref, k_ref, v_ref, u_ref, rk_ref, lf_ref, *refs):
    outs = refs[deps:]
    spans = [slice(c * MBLOCK, (c + 1) * MBLOCK) for c in range(q_ref.shape[0] // MBLOCK)]
    results = prepare_chunks(
        [q_ref[s].astype(FLOAT32) for s in spans], [k_ref[s].astype(FLOAT32) for s in spans],
        [v_ref[s] for s in spans], [u_ref[s] for s in spans], [rk_ref[s] for s in spans],
        [lf_ref[s] for s in spans])
    for ref, values in zip(outs, results):
        for s, value in zip(spans, values):
            ref[s] = value


def prepare(inputs, start, count, deps):
    width = inputs[0].shape[1]
    tile = count * MBLOCK
    spec = pl.BlockSpec((tile, width), lambda i: (start // count, 0))
    full = jax.ShapeDtypeStruct((tile, width), FLOAT32)
    return pl.pallas_call(
        functools.partial(prepare_kernel, len(deps)),
        grid=(1,),
        out_shape=[full] * 4,
        in_specs=[spec] * 6 + after(deps, len(deps)),
        out_specs=[pl.BlockSpec((tile, width), lambda i: (0, 0))] * 4,
        name="prepare",
    )(*inputs, *deps)


def head_mean(value, same):
    high, low = parts2(value)
    return dot(jnp.concatenate([high, low], axis=1), same) * (1.0 / RHEAD)


def scan_kernel(deps, pieces, gain_ref, *refs):
    prepared = [refs[4 * p : 4 * p + 4] for p in range(pieces)]
    out_ref, raw_ref = refs[4 * pieces + deps :]
    width = out_ref.shape[1]
    same = (iota((width, width), 0) // RHEAD == iota((width, width), 1) // RHEAD).astype(BFLOAT)
    same = jnp.concatenate([same, same], axis=0)
    state = None
    done = 0
    for qe_ref, ob_ref, st_ref, ad_ref in prepared:
        for c in range(qe_ref.shape[0] // MBLOCK):
            rows = slice(c * MBLOCK, (c + 1) * MBLOCK)
            out = ob_ref[rows, :]
            if state is None:
                state = ad_ref[rows, :]
            else:
                out = out + dot(left_of(qe_ref[rows, :]), right_nt(state), NT)
                state = dot(left_of(state), right_of(st_ref[rows, :])) + ad_ref[rows, :]
            raw_ref[done : done + MBLOCK, :] = out
            done += MBLOCK
    raw = raw_ref[...]
    centred = raw - head_mean(raw, same)
    var = head_mean(centred * centred, same)
    out_ref[...] = (centred * lax.rsqrt(var + 0.00064) * gain_ref[...]).astype(BFLOAT)


def scan(prepared, norm_gain, deps):
    width = prepared[0][0].shape[1]
    rows = sum(p[0].shape[0] for p in prepared)
    flat = [a for p in prepared for a in p]
    return pl.pallas_call(
        functools.partial(scan_kernel, len(deps), len(prepared)),
        out_shape=jax.ShapeDtypeStruct((rows, width), BFLOAT),
        in_specs=whole(1 + len(flat)) + after(deps, len(deps)),
        out_specs=pl.BlockSpec(memory_space=VMEM),
        scratch_shapes=[VMEM((rows, width), FLOAT32)],
        name="scan",
    )(norm_gain.reshape(1, -1), *flat, *deps)


def attend_group(plen, q_ref, k_ref, v_ref, out_ref):
    width = q_ref.shape[1]
    heads = width // XHEAD
    capacity = (q_ref.shape[0] - LROWS) // QBLOCK
    line = q_ref[capacity * QBLOCK :, :128].astype(FLOAT32)
    units = [(r, h) for r in range(capacity) for h in range(heads)]
    spans = [pl.ds(pl.multiple_of(entry(line, 0, r) * plen, plen), plen) for r in range(capacity)]
    mine = [slice(r * QBLOCK, (r + 1) * QBLOCK) for r in range(capacity)]
    cols = [slice(h * XHEAD, (h + 1) * XHEAD) for h in range(heads)]
    scores = [dot(q_ref[mine[r], cols[h]], k_ref[spans[r], cols[h]], NT) for r, h in units]
    expon = [jnp.exp(s * XHEAD ** (-0.5)).astype(BFLOAT) for s in scores]
    ones = jnp.ones((8, plen), BFLOAT)
    totals = [dot(ones, e, NT)[:1] for e in expon]
    outs = [dot(e, v_ref[spans[r], cols[h]]) for e, (r, h) in zip(expon, units)]
    sums = jnp.zeros((LROWS, QBLOCK), FLOAT32)
    rowid = iota((LROWS, QBLOCK), 0)
    for (r, h), out, total in zip(units, outs, totals):
        out_ref[mine[r], cols[h]] = out.astype(BFLOAT)
        high = total.astype(BFLOAT).astype(FLOAT32)
        where = 2 * (r * heads + h)
        sums = jnp.where(rowid == where, high, sums)
        sums = jnp.where(rowid == where + 1, total - high, sums)
    out_ref[capacity * QBLOCK :, :] = jnp.zeros((LROWS, width), BFLOAT)
    out_ref[capacity * QBLOCK :, :QBLOCK] = sums.astype(BFLOAT)


def attend_kernel(plen, count, deps, k_ref, v_ref, *refs):
    for q_ref, out_ref in zip(refs[:count], refs[count + deps :]):
        attend_group(plen, q_ref, k_ref, v_ref, out_ref)


def attend(groups, keys, values, plen, deps):
    count = len(groups)
    return pl.pallas_call(
        functools.partial(attend_kernel, plen, count, len(deps)),
        out_shape=[jax.ShapeDtypeStruct(g.shape, BFLOAT) for g in groups],
        in_specs=whole(2 + count) + after(deps, len(deps)),
        out_specs=whole(count),
        name="attend",
    )(keys, values, *groups, *deps)


def add_group(blocks, part_ref, acc_ref, den_ref):
    width = part_ref.shape[1]
    heads = width // XHEAD
    qrows = part_ref.shape[0] - LROWS
    lines = part_ref[qrows:, :QBLOCK].astype(FLOAT32)
    for r, block in enumerate(blocks):
        @pl.when(block > 0)
        def _(r=r, block=block):
            rows = pl.ds(pl.multiple_of((block - 1) * QBLOCK, QBLOCK), QBLOCK)
            acc_ref[rows, :] += part_ref[r * QBLOCK : (r + 1) * QBLOCK, :].astype(FLOAT32)
            for h in range(heads):
                at = 2 * (r * heads + h)
                den_ref[pl.ds((block - 1) * heads + h, 1), :] += lines[at : at + 1] + lines[at + 1 : at + 2]


def gather_kernel(count, deps, me_ref, blk_ref, *refs):
    parts = refs[:count]
    out_ref, acc_ref, den_ref = refs[count + deps :]
    capacity = blk_ref.shape[1]
    acc_ref[...] = jnp.zeros_like(acc_ref)
    den_ref[...] = jnp.zeros_like(den_ref)
    for k, part_ref in enumerate(parts):
        owner = me_ref[0] ^ k
        add_group([blk_ref[owner, r] for r in range(capacity)], part_ref, acc_ref, den_ref)
    rows = acc_ref.shape[0]
    lines = den_ref.shape[0]
    out_ref[:rows, :] = acc_ref[...].astype(BFLOAT)
    out_ref[rows:, :] = jnp.zeros((out_ref.shape[0] - rows, out_ref.shape[1]), BFLOAT)
    high, low = parts2(den_ref[...])
    out_ref[rows : rows + lines, :QBLOCK] = high
    out_ref[rows : rows + lines, 128 : 128 + QBLOCK] = low


def gather(me, blk, parts, rows, deps):
    width = parts[0].shape[1]
    lines = up16(rows // QBLOCK * (width // XHEAD))
    smem = pl.BlockSpec(memory_space=SMEM)
    return pl.pallas_call(
        functools.partial(gather_kernel, len(parts), len(deps)),
        out_shape=jax.ShapeDtypeStruct((rows + lines, width), BFLOAT),
        in_specs=[smem, smem] + whole(len(parts)) + after(deps, len(deps)),
        out_specs=pl.BlockSpec(memory_space=VMEM),
        scratch_shapes=[VMEM((rows, width), FLOAT32), VMEM((lines, QBLOCK), FLOAT32)],
        name="gather",
    )(me, blk, *parts, *deps)


def combine_kernel(count, deps, me_ref, blk_ref, far_ref, *refs):
    parts = refs[:count]
    out_ref, acc_ref, den_ref = refs[count + deps :]
    capacity = blk_ref.shape[1]
    rows, width = acc_ref.shape
    heads = width // XHEAD
    lines = den_ref.shape[0]
    acc_ref[...] = far_ref[:rows, :].astype(FLOAT32)
    tail = far_ref[rows : rows + lines, :].astype(FLOAT32)
    den_ref[...] = tail[:, :QBLOCK] + tail[:, 128 : 128 + QBLOCK]
    for k, part_ref in enumerate(parts):
        owner = me_ref[0] ^ k
        add_group([blk_ref[owner, r] for r in range(capacity)], part_ref, acc_ref, den_ref)
    turned = jnp.transpose(den_ref[...])
    for b in range(rows // QBLOCK):
        mine = slice(b * QBLOCK, (b + 1) * QBLOCK)
        for h in range(heads):
            cols = slice(h * XHEAD, (h + 1) * XHEAD)
            at = b * heads + h
            out_ref[mine, cols] = (acc_ref[mine, cols] / turned[:, at : at + 1]).astype(BFLOAT)


def combine(me, blk, far, parts, rows, deps):
    width = far.shape[1]
    smem = pl.BlockSpec(memory_space=SMEM)
    return pl.pallas_call(
        functools.partial(combine_kernel, len(parts), len(deps)),
        out_shape=jax.ShapeDtypeStruct((rows, width), BFLOAT),
        in_specs=[smem, smem] + whole(1 + len(parts)) + after(deps, len(deps)),
        out_specs=pl.BlockSpec(memory_space=VMEM),
        scratch_shapes=[VMEM((rows, width), FLOAT32), VMEM((far.shape[0] - rows, QBLOCK), FLOAT32)],
        name="combine",
    )(me, blk, far, *parts, *deps)


def gathered_dot(pieces, me, w_ref):
    total = None
    for j, piece in enumerate(pieces):
        depth = piece.shape[1]
        rows = pl.ds(pl.multiple_of((me ^ j) * depth, depth), depth)
        part = dot(piece[...], w_ref[rows, :])
        total = part if total is None else total + part
    return total


def mixer_out_kernel(me_ref, *refs):
    *pieces, w_ref, out_ref = refs
    out_ref[...] = gathered_dot(pieces, me_ref[0], w_ref)


def final_kernel(me_ref, *refs):
    *pieces, w_ref, gate_ref, mixer_ref, out_ref = refs
    cross = gathered_dot(pieces, me_ref[0], w_ref)
    out_ref[...] = (mixer_ref[...] + gate_ref[...] * cross).astype(BFLOAT)


def over_tp(body, me, pieces, others, dtype, name):
    shape = (pieces[0].shape[0], others[0].shape[1])
    return pl.pallas_call(
        body,
        out_shape=jax.ShapeDtypeStruct(shape, dtype),
        in_specs=[pl.BlockSpec(memory_space=SMEM)] + whole(len(pieces) + len(others)),
        out_specs=pl.BlockSpec(memory_space=VMEM),
        name=name,
    )(me, *pieces, *others)


def gather_tp(piece, count):
    pieces = {0: piece}
    bit = count // 2
    while bit:
        pairs = [(i, i ^ bit) for i in range(count)]
        for j in list(pieces):
            pieces[j ^ bit] = lax.ppermute(pieces[j], "tp", pairs)
        bit //= 2
    return [pieces[j] for j in range(count)]


def local(
    tokens, mix_query, mix_key, mix_value, decay_lower_map, decay_upper_map, decay_base,
    decay_shift, rate_lower_map, rate_upper_map, norm_gain, mix_out, cross_query, score_gain,
    passage_key, passage_value, cross_out, gate_down, gate_up, store, passage_ids,
):
    rows = tokens.shape[0]
    owners = lax.axis_size("st")
    shards = lax.axis_size("tp")
    pass_dev, plen, _ = store.shape
    per_block = passage_ids.shape[1]
    slots = passage_ids.shape[0] * per_block
    capacity = max(2, -(-slots // owners))
    me = lax.axis_index("tp").astype(jnp.int32).reshape(1)
    place = lax.axis_index("st").astype(jnp.int32).reshape(1)
    half = owners // 2

    def swap(value, bit):
        return lax.ppermute(value, "st", [(i, i ^ bit) for i in range(owners)])

    def swap_groups(groups):
        return [groups[0]] + [swap(groups[k], k) for k in range(1, half)]

    queries, blk, near = make_queries(
        place, passage_ids, owners, capacity, pass_dev, tokens, cross_query, score_gain)
    far_queries = swap(queries, half)
    near = swap_groups(near)
    keys, values = make_keyvals(store, passage_key, passage_value)
    *mixer_in, gate = project(
        tokens, mix_query, mix_key, mix_value, decay_lower_map, decay_upper_map, decay_base,
        decay_shift, rate_lower_map, rate_upper_map, gate_down, gate_up)
    chunks = rows // MBLOCK
    pieces = [(0, 3), (3, 3), (6, 2)] if chunks == 8 else [(c, 1) for c in range(chunks)]
    early, *others, last = pieces
    prepared = [prepare(mixer_in, *early, [keys])]
    far_blk, far = relay(place, far_queries, rows, owners, capacity, [prepared[-1][0]])
    far = swap_groups(far)
    near_parts = attend(near, keys, values, plen, [far[0]])
    for piece in others:
        prepared.append(prepare(mixer_in, *piece, [near_parts[0]]))
    far_parts = attend(far, keys, values, plen, [prepared[-1][0]])
    prepared.append(prepare(mixer_in, *last, [far_parts[0]]))
    far_parts = swap_groups(far_parts)
    returned = gather(place, far_blk, far_parts, rows, [prepared[-1][0]])
    near_parts, returned = lax.optimization_barrier((near_parts, returned))
    returned = swap(returned, half)
    near_parts = swap_groups(near_parts)
    mixer_heads = scan(prepared, norm_gain, [])
    mixer_all = gather_tp(mixer_heads, shards)
    attended = combine(place, blk, returned, near_parts, rows, [mixer_heads])
    mixer_part = over_tp(mixer_out_kernel, me, mixer_all, [mix_out], FLOAT32, "mixer_out")
    return over_tp(final_kernel, me, gather_tp(attended, shards), [cross_out, gate, mixer_part],
                   BFLOAT, "final")


def solution(mesh):
    placed = (
        P("st", None), P(None, "tp"), P(None, "tp"), P(None, "tp"), P(), P(None, "tp"), P("tp"),
        P("st", "tp"), P(), P(None, "tp"), P("tp"), P(None, "tp"), P(None, "tp"), P("tp"),
        P(None, "tp"), P(None, "tp"), P(None, "tp"), P(), P(None, "tp"), P("st", None, None),
        P("st", None),
    )
    return jax.shard_map(
        local, mesh=mesh, in_specs=placed, out_specs=P("st", "tp"), check_vma=False
    )
```

```python
import functools
import jax
import jax.numpy as jnp
from jax import lax
from jax.experimental import pallas as pl
from jax.experimental.pallas import tpu as pltpu
from jax.sharding import PartitionSpec as P


XHEAD = 256
QBLOCK = 64
MBLOCK = 64
RHEAD = 64
LROWS = 16

FLOAT32 = jnp.float32
BFLOAT = jnp.bfloat16
PRECISE = lax.Precision.HIGHEST
VMEM = pltpu.VMEM
SMEM = pltpu.SMEM
GRANT = pltpu.CompilerParams(vmem_limit_bytes=14 * 1024 * 1024)
NT = (((1,), (1,)), ((), ()))
NN = (((1,), (0,)), ((), ()))
TN = (((0,), (0,)), ((), ()))


def dot(left, right, dims=NN, precision=None):
    return lax.dot_general(left, right, dims, precision=precision, preferred_element_type=FLOAT32)


def iota(shape, dim):
    return lax.broadcasted_iota(jnp.int32, shape, dim)


def whole(count):
    return [pl.BlockSpec(memory_space=VMEM)] * count


def in_hbm(*arrays):
    return [pltpu.with_memory_space_constraint(a, pltpu.HBM) for a in arrays]


def near_core(*arrays):
    return [pltpu.with_memory_space_constraint(a, VMEM) for a in arrays]


def after(count):
    return [pl.BlockSpec(memory_space=pl.ANY)] * count


def up16(count):
    return -(-count // 16) * 16


def entry(lines, row, lane):
    hit = (iota(lines.shape, 0) == row) & (iota(lines.shape, 1) == lane)
    return jnp.sum(jnp.where(hit, lines, 0.0)).astype(jnp.int32)


def write_group(out_ref, q_ref, blocks, passages):
    capacity = len(blocks)
    width = out_ref.shape[1]
    line = jnp.zeros((LROWS, width), FLOAT32)
    row, lane = iota(line.shape, 0), iota(line.shape, 1)
    for r in range(capacity):
        start = pl.multiple_of(jnp.maximum(blocks[r] - 1, 0) * QBLOCK, QBLOCK)
        out_ref[r * QBLOCK : (r + 1) * QBLOCK, :] = q_ref[pl.ds(start, QBLOCK), :]
        line = jnp.where((row == 0) & (lane == r), passages[r].astype(FLOAT32), line)
    out_ref[capacity * QBLOCK :, :] = line.astype(BFLOAT)


def query_kernel(pass_dev, owners, me_ref, ids_ref, tok_ref, w_ref, gain_ref, blk_ref, *refs):
    capacity = blk_ref.shape[1]
    per_block = ids_ref.shape[0]
    rows, width = tok_ref.shape[0], w_ref.shape[1]
    heads = width // XHEAD
    q_refs, group_refs = refs[:heads], refs[heads:-4]
    pidx_ref, fill_ref, sum_ref, all_ref = refs[-4:]
    step = pl.program_id(0)

    @pl.when(step == 0)
    def _():
        def clear(o, carry):
            fill_ref[o] = 0
            for r in range(capacity):
                pidx_ref[o, r] = 0
                blk_ref[o, r] = 0
            return carry

        lax.fori_loop(0, owners, clear, 0)

        def put(n, carry):
            passage = ids_ref[n % per_block, n // per_block]
            owner = passage // pass_dev
            rank = fill_ref[owner]
            fill_ref[owner] = rank + 1
            pidx_ref[owner, rank] = passage - owner * pass_dev
            blk_ref[owner, rank] = n // per_block + 1
            return carry

        lax.fori_loop(0, ids_ref.shape[1] * per_block, put, 0)
        sum_ref[...] = jnp.zeros_like(sum_ref)

    sum_ref[...] += dot(tok_ref[...], w_ref[...])

    @pl.when(step == pl.num_programs(0) - 1)
    def _():
        tail = q_refs[0].shape[0] - rows
        row, lane = iota((tail, 128), 0), iota((tail, 128), 1)

        def line(o, table):
            for r in range(capacity):
                table = jnp.where((row == o) & (lane == r), blk_ref[o, r].astype(FLOAT32), table)
                table = jnp.where((row == o) & (lane == capacity + r),
                                  pidx_ref[o, r].astype(FLOAT32), table)
            return table

        table = lax.fori_loop(0, owners, line, jnp.zeros((tail, 128), FLOAT32)).astype(BFLOAT)
        for h, q_ref in enumerate(q_refs):
            cols = slice(h * XHEAD, (h + 1) * XHEAD)
            raw = sum_ref[:, cols]
            scale = lax.rsqrt(jnp.mean(raw * raw, axis=-1, keepdims=True) + 1e-06)
            value = (raw * scale * gain_ref[:, cols]).astype(BFLOAT)
            q_ref[:rows, :] = value
            all_ref[:, cols] = value
            q_ref[rows:, :] = jnp.concatenate([table, jnp.zeros_like(table)], axis=1)
        for k, ref in enumerate(group_refs):
            owner = me_ref[0] ^ k
            write_group(ref, all_ref, [blk_ref[owner, r] for r in range(capacity)],
                        [pidx_ref[owner, r] for r in range(capacity)])


def make_queries(me, ids, owners, capacity, pass_dev, tokens, cross_query, score_gain):
    rows, width = tokens.shape[0], cross_query.shape[1]
    smem = pl.BlockSpec(memory_space=SMEM)
    group = VMEM((capacity * QBLOCK + LROWS, width), BFLOAT)
    count, heads = owners // 2, width // XHEAD
    steps = 4
    depth = tokens.shape[1] // steps
    outs = pl.pallas_call(
        functools.partial(query_kernel, pass_dev, owners),
        grid=(steps,),
        out_shape=[jax.ShapeDtypeStruct((owners, capacity), jnp.int32)]
        + [VMEM((rows + up16(owners), XHEAD), BFLOAT)] * heads + [group] * count,
        in_specs=[smem, smem, pl.BlockSpec((rows, depth), lambda i: (0, i)),
                  pl.BlockSpec((depth, width), lambda i: (i, 0))] + whole(1),
        out_specs=[smem] + whole(heads + count),
        scratch_shapes=[SMEM((owners, capacity), jnp.int32), SMEM((owners,), jnp.int32),
                        VMEM((rows, width), FLOAT32), VMEM((rows, width), BFLOAT)],
        compiler_params=GRANT,
        name="queries",
    )(me, *in_hbm(ids.T, tokens, cross_query, score_gain.reshape(1, -1)))
    return outs[0], outs[1 : 1 + heads], outs[1 + heads :]


def relay_kernel(rows, deps, me_ref, q_ref, *refs):
    blk_ref, *group_refs = refs[deps:]
    _, capacity = blk_ref.shape
    table = q_ref[rows:, :128].astype(FLOAT32)
    for k, ref in enumerate(group_refs):
        owner = me_ref[0] ^ k
        blocks = [entry(table, owner, r) for r in range(capacity)]
        for r in range(capacity):
            blk_ref[owner, r] = blocks[r]
        write_group(ref, q_ref, blocks, [entry(table, owner, capacity + r) for r in range(capacity)])


def relay(me, queries, rows, owners, capacity, deps):
    width = queries.shape[1]
    smem = pl.BlockSpec(memory_space=SMEM)
    group = VMEM((capacity * QBLOCK + LROWS, width), BFLOAT)
    count = owners // 2
    outs = pl.pallas_call(
        functools.partial(relay_kernel, rows, len(deps)),
        out_shape=[jax.ShapeDtypeStruct((owners, capacity), jnp.int32)] + [group] * count,
        in_specs=[smem] + whole(1) + after(len(deps)),
        out_specs=[smem] + whole(count),
        compiler_params=GRANT,
        name="relay",
    )(me, *near_core(queries), *deps)
    return outs[0], outs[1:]


def keyval_kernel(rows_ref, wk_ref, wv_ref, k_ref, v_ref):
    width = wk_ref.shape[1]
    rows = rows_ref[...]
    mine = pl.ds(pl.multiple_of(pl.program_id(0) * rows.shape[0], 16), rows.shape[0])
    for h in range(width // XHEAD):
        cols = slice(h * XHEAD, (h + 1) * XHEAD)
        raw = dot(rows, wk_ref[:, cols])
        scale = lax.rsqrt(jnp.mean(raw * raw, axis=-1, keepdims=True) + 1e-06)
        k_ref[mine, cols] = (raw * scale).astype(BFLOAT)
        v_ref[mine, cols] = dot(rows, wv_ref[:, cols]).astype(BFLOAT)


def make_keyvals(store, passage_key, passage_value):
    pass_dev, plen, model = store.shape
    width = passage_key.shape[1]
    group = max(g for g in range(1, 5) if pass_dev % g == 0)
    tile = group * plen
    shape = VMEM((pass_dev * plen, width), BFLOAT)
    return pl.pallas_call(
        keyval_kernel,
        grid=(pass_dev // group,),
        out_shape=[shape, shape],
        in_specs=[pl.BlockSpec((tile, model), lambda i: (i, 0))] + whole(2),
        out_specs=whole(2),
        compiler_params=GRANT,
        name="keyvals",
    )(*in_hbm(store.reshape(-1, model)), *near_core(passage_key, passage_value))


def project_kernel(
    tok_ref, mq_ref, mk_ref, mv_ref, dl_ref, rl_ref, gd_ref, du_ref, ru_ref, gu_ref,
    base_ref, shift_ref, dep_ref,
    q_ref, k_ref, v_ref, u_ref, rk_ref, lf_ref, gate_ref,
):
    tokens = tok_ref[...]
    width = mq_ref.shape[1]
    rank = dl_ref.shape[0]
    lows = dot(tokens, jnp.concatenate([dl_ref[...], rl_ref[...]], axis=0), NT)
    decay_low = jnp.tanh(lows[:, :rank]).astype(BFLOAT)
    rate_low = lows[:, rank:].astype(BFLOAT)
    gate_low = dot(tokens, gd_ref[...]).astype(BFLOAT)
    gate_ref[...] = jax.nn.sigmoid(dot(gate_low, gu_ref[...]))
    pre = base_ref[...] + dot(decay_low, du_ref[...])
    heads = shift_ref.shape[0]
    owner = (iota((heads, width), 0) == iota((heads, width), 1) // RHEAD).astype(FLOAT32)
    shift = dot(shift_ref[...], owner, TN, precision=PRECISE)
    lf_ref[...] = -jax.nn.sigmoid(pre + shift) * (2.718281828459045 ** -0.5)
    q_ref[...] = dot(tokens, mq_ref[...]).astype(BFLOAT)
    v_ref[...] = dot(tokens, mv_ref[...]).astype(BFLOAT)
    key = dot(tokens, mk_ref[...]).astype(BFLOAT)
    k_ref[...] = key
    key = key.astype(FLOAT32)
    same = (iota((width, width), 0) // RHEAD == iota((width, width), 1) // RHEAD).astype(FLOAT32)
    unit = key * lax.rsqrt(dot(key * key, same, precision=PRECISE) + 1e-06)
    u_ref[...] = unit
    rk_ref[...] = unit * jax.nn.sigmoid(dot(rate_low, ru_ref[...]))


def project(tokens, mix_query, mix_key, mix_value, decay_lower, decay_upper, decay_base,
            decay_shift, rate_lower, rate_upper, gate_down, gate_up, deps):
    rows = tokens.shape[0]
    width = mix_query.shape[1]
    half = VMEM((rows, width), BFLOAT)
    full = VMEM((rows, width), FLOAT32)
    return pl.pallas_call(
        project_kernel,
        out_shape=[half, half, half, full, full, full,
                   VMEM((rows, gate_up.shape[1]), FLOAT32)],
        in_specs=whole(12) + after(len(deps)),
        out_specs=whole(7),
        compiler_params=GRANT,
        name="project",
    )(*near_core(tokens, mix_query, mix_key, mix_value), decay_lower.T, rate_lower.T, gate_down,
      decay_upper, rate_upper, gate_up, decay_base.reshape(1, -1), decay_shift.T, *deps)


def parts2(value):
    high = value.astype(BFLOAT)
    return high, (value - high.astype(FLOAT32)).astype(BFLOAT)


def parts3(value):
    high = value.astype(BFLOAT)
    rest = value - high.astype(FLOAT32)
    return (high,) + parts2(rest)


def spread(value):
    rows, width = value.shape
    lane = iota((1, 128), 1) // RHEAD
    blank = jnp.zeros((rows, 128), value.dtype)
    blocks = []
    for h in range(width // RHEAD):
        mine = (h * RHEAD) // 128
        keep = (lane == h % (128 // RHEAD)).astype(value.dtype)
        cells = [blank] * (width // 128)
        cells[mine] = value[:, mine * 128 : (mine + 1) * 128] * keep
        blocks.append(jnp.concatenate(cells, axis=1) if len(cells) > 1 else cells[0])
    return jnp.concatenate(blocks, axis=0)


def fold(value):
    width = value.shape[1]
    lane = iota((1, 128), 1) // RHEAD
    cells = []
    for t in range(width // 128):
        cell = value[t * 128 : t * 128 + RHEAD, t * 128 : (t + 1) * 128]
        for p in range(1, 128 // RHEAD):
            start = t * 128 + p * RHEAD
            cell = jnp.where(lane == p, value[start : start + RHEAD, t * 128 : (t + 1) * 128], cell)
        cells.append(cell)
    return jnp.concatenate(cells, axis=1) if len(cells) > 1 else cells[0]


def left_of(value):
    high, low = parts2(value)
    return jnp.concatenate([high, low, high], axis=1)


def right_of(value):
    high, low = parts2(value)
    high, low = spread(high), spread(low)
    return jnp.concatenate([high, high, low], axis=0)


def right_nt(value):
    high, low = parts2(value)
    high, low = spread(high), spread(low)
    return jnp.concatenate([high, high, low], axis=1)


def across(left, right):
    lh, ll = parts2(left)
    rh, rl = parts2(right)
    return fold(dot(jnp.concatenate([lh, ll, lh], axis=0), jnp.concatenate([rh, rh, rl], axis=0), TN))


def prepare_chunks(queries, keys, values, units, rate_keys, fades):
    n = range(len(queries))
    length, width = queries[0].shape
    row = iota((length, width), 0)
    col = iota((length, width), 1) % RHEAD
    lower = (iota((length, length), 1) <= iota((length, length), 0)).astype(BFLOAT)
    cumul = []
    for c in n:
        sums = dot(lower, jnp.concatenate(parts3(fades[c]), axis=1))
        cumul.append(sums[:, :width] + sums[:, width : 2 * width] + sums[:, 2 * width :])
    ends = [cumul[c][length - 1 :, :] for c in n]
    grown = [jnp.exp(-cumul[c]) for c in n]
    pulled = [-units[c] * jnp.exp(cumul[c] - fades[c]) for c in n]
    read = [queries[c] * jnp.exp(cumul[c]) for c in n]
    both = [left_of(jnp.concatenate([pulled[c], read[c]], axis=0)) for c in n]
    from_rate = [dot(both[c], right_nt(rate_keys[c] * grown[c]), NT) for c in n]
    from_key = [dot(both[c], right_nt(keys[c] * grown[c]), NT) for c in n]
    strict, upto = col < row, col <= row
    rate_pull = [jnp.where(strict, from_rate[c][:length], 0.0) for c in n]
    rate_read = [left_of(jnp.where(upto, from_rate[c][length:], 0.0)) for c in n]
    key_both = [
        left_of(jnp.concatenate([jnp.where(strict, from_key[c][:length], 0.0),
                                 jnp.where(upto, from_key[c][length:], 0.0)], axis=0)) for c in n]

    def pick(size):
        return (row // (2 * size) == col // (2 * size)) & (row // size > col // size)

    first = pick(1)
    eye = (row == col).astype(FLOAT32)
    inverse = [eye + jnp.where(first, rate_pull[c], 0.0) for c in n]
    size = 2
    while size < length:
        keep = pick(size)
        mids = [dot(left_of(inverse[c]), right_of(jnp.where(keep, rate_pull[c], 0.0))) for c in n]
        adds = [dot(left_of(mids[c]), right_of(inverse[c])) for c in n]
        inverse = [inverse[c] + adds[c] for c in n]
        size *= 2
    inverse = [left_of(inverse[c]) for c in n]
    from_value = []
    for c in n:
        wide = spread(values[c])
        from_value.append(dot(key_both[c][:, : 2 * width], jnp.concatenate([wide, wide], axis=0)))
    moved = [dot(inverse[c], right_of(pulled[c])) for c in n]
    base = [dot(inverse[c], right_of(from_value[c][:length])) for c in n]
    query_end = [read[c] + dot(rate_read[c], right_of(moved[c])) for c in n]
    out_base = [from_value[c][length:] + dot(rate_read[c], right_of(base[c])) for c in n]
    left = [jnp.exp(ends[c] - cumul[c]) for c in n]
    step, add = [], []
    diag = iota((RHEAD, width), 0) == iota((RHEAD, width), 1) % RHEAD
    for c in n:
        rate_left = rate_keys[c] * left[c]
        step.append(jnp.where(diag, jnp.exp(ends[c]), 0.0) + across(moved[c], rate_left))
        add.append(across(jnp.concatenate([values[c].astype(FLOAT32), base[c]], axis=0),
                          jnp.concatenate([keys[c] * left[c], rate_left], axis=0)))
    return query_end, out_base, step, add


def prepare_kernel(start, deps, q_ref, k_ref, v_ref, u_ref, rk_ref, lf_ref, *refs):
    outs = refs[deps:]
    count = outs[0].shape[0] // MBLOCK
    spans = [slice((start + c) * MBLOCK, (start + c + 1) * MBLOCK) for c in range(count)]
    results = prepare_chunks(
        [q_ref[s].astype(FLOAT32) for s in spans], [k_ref[s].astype(FLOAT32) for s in spans],
        [v_ref[s] for s in spans], [u_ref[s] for s in spans], [rk_ref[s] for s in spans],
        [lf_ref[s] for s in spans])
    for ref, values in zip(outs, results):
        for c, value in enumerate(values):
            ref[c * MBLOCK : (c + 1) * MBLOCK] = value


def prepare(inputs, start, count, deps):
    width = inputs[0].shape[1]
    full = VMEM((count * MBLOCK, width), FLOAT32)
    return pl.pallas_call(
        functools.partial(prepare_kernel, start, len(deps)),
        out_shape=[full] * 4,
        in_specs=whole(6) + after(len(deps)),
        out_specs=whole(4),
        compiler_params=GRANT,
        name="prepare",
    )(*near_core(*inputs), *deps)


def head_mean(value, same):
    high, low = parts2(value)
    return dot(jnp.concatenate([high, low], axis=1), same) * (1.0 / RHEAD)


def scan_kernel(deps, pieces, gain_ref, *refs):
    prepared = [refs[4 * p : 4 * p + 4] for p in range(pieces)]
    out_ref, raw_ref = refs[4 * pieces + deps :]
    width = out_ref.shape[1]
    same = (iota((width, width), 0) // RHEAD == iota((width, width), 1) // RHEAD).astype(BFLOAT)
    same = jnp.concatenate([same, same], axis=0)
    state = None
    done = 0
    for qe_ref, ob_ref, st_ref, ad_ref in prepared:
        for c in range(qe_ref.shape[0] // MBLOCK):
            rows = slice(c * MBLOCK, (c + 1) * MBLOCK)
            out = ob_ref[rows, :]
            if state is None:
                state = ad_ref[rows, :]
            else:
                out = out + dot(left_of(qe_ref[rows, :]), right_nt(state), NT)
                state = dot(left_of(state), right_of(st_ref[rows, :])) + ad_ref[rows, :]
            raw_ref[done : done + MBLOCK, :] = out
            done += MBLOCK
    raw = raw_ref[...]
    centred = raw - head_mean(raw, same)
    var = head_mean(centred * centred, same)
    out_ref[...] = (centred * lax.rsqrt(var + 0.00064) * gain_ref[...]).astype(BFLOAT)


def scan(prepared, norm_gain, deps):
    width = prepared[0][0].shape[1]
    rows = sum(p[0].shape[0] for p in prepared)
    flat = [a for p in prepared for a in p]
    return pl.pallas_call(
        functools.partial(scan_kernel, len(deps), len(prepared)),
        out_shape=VMEM((rows, width), BFLOAT),
        in_specs=whole(1 + len(flat)) + after(len(deps)),
        out_specs=pl.BlockSpec(memory_space=VMEM),
        scratch_shapes=[VMEM((rows, width), FLOAT32)],
        compiler_params=GRANT,
        name="scan",
    )(norm_gain.reshape(1, -1), *near_core(*flat), *deps)


def attend_group(plen, first, q_ref, k_ref, v_ref, out_ref):
    width = q_ref.shape[1]
    heads = width // XHEAD
    capacity = (q_ref.shape[0] - LROWS) // QBLOCK
    line = q_ref[capacity * QBLOCK :, :128].astype(FLOAT32)
    units = [(r, h) for r in range(capacity) for h in range(heads)]
    spans = [pl.ds(pl.multiple_of(entry(line, 0, r) * plen, plen), plen) for r in range(capacity)]
    mine = [slice(r * QBLOCK, (r + 1) * QBLOCK) for r in range(capacity)]
    cols = [slice(h * XHEAD, (h + 1) * XHEAD) for h in range(heads)]
    held = [slice((first + h) * XHEAD, (first + h + 1) * XHEAD) for h in range(heads)]
    scores = [dot(q_ref[mine[r], cols[h]], k_ref[spans[r], held[h]], NT) for r, h in units]
    expon = [jnp.exp(s * XHEAD ** (-0.5)).astype(BFLOAT) for s in scores]
    ones = jnp.ones((8, plen), BFLOAT)
    totals = [dot(ones, e, NT)[:1] for e in expon]
    outs = [dot(e, v_ref[spans[r], held[h]]) for e, (r, h) in zip(expon, units)]
    sums = jnp.zeros((LROWS, QBLOCK), FLOAT32)
    rowid = iota((LROWS, QBLOCK), 0)
    for (r, h), out, total in zip(units, outs, totals):
        out_ref[mine[r], cols[h]] = out.astype(BFLOAT)
        high = total.astype(BFLOAT).astype(FLOAT32)
        where = 2 * (r * heads + h)
        sums = jnp.where(rowid == where, high, sums)
        sums = jnp.where(rowid == where + 1, total - high, sums)
    out_ref[capacity * QBLOCK :, :] = jnp.zeros((LROWS, width), BFLOAT)
    out_ref[capacity * QBLOCK :, :QBLOCK] = sums.astype(BFLOAT)


def attend_kernel(plen, first, count, deps, k_ref, v_ref, *refs):
    for q_ref, out_ref in zip(refs[:count], refs[count + deps :]):
        attend_group(plen, first, q_ref, k_ref, v_ref, out_ref)


def attend(groups, keys, values, plen, first, deps):
    count = len(groups)
    return pl.pallas_call(
        functools.partial(attend_kernel, plen, first, count, len(deps)),
        out_shape=[VMEM(g.shape, BFLOAT) for g in groups],
        in_specs=whole(2 + count) + after(len(deps)),
        out_specs=whole(count),
        compiler_params=GRANT,
        name="attend",
    )(*near_core(keys, values, *groups), *deps)


def add_group(blocks, head, part_ref, acc_ref, den_ref):
    heads = part_ref.shape[1] // XHEAD
    qrows = part_ref.shape[0] - LROWS
    lines = part_ref[qrows:, :QBLOCK].astype(FLOAT32)
    cols = slice(head * XHEAD, (head + 1) * XHEAD)
    for r, block in enumerate(blocks):
        @pl.when(block > 0)
        def _(r=r, block=block):
            rows = pl.ds(pl.multiple_of((block - 1) * QBLOCK, QBLOCK), QBLOCK)
            acc_ref[rows, :] += part_ref[r * QBLOCK : (r + 1) * QBLOCK, cols].astype(FLOAT32)
            at = 2 * (r * heads + head)
            den_ref[pl.ds(block - 1, 1), :] += lines[at : at + 1] + lines[at + 1 : at + 2]


def gather_kernel(count, deps, me_ref, blk_ref, *refs):
    parts = refs[:count]
    out_ref, acc_ref, den_ref = refs[count + deps :]
    capacity = blk_ref.shape[1]
    acc_ref[...] = jnp.zeros_like(acc_ref)
    den_ref[...] = jnp.zeros_like(den_ref)
    for k, part_ref in enumerate(parts):
        owner = me_ref[0] ^ k
        add_group([blk_ref[owner, r] for r in range(capacity)], 0, part_ref, acc_ref, den_ref)
    rows, lines = acc_ref.shape[0], den_ref.shape[0]
    out_ref[:rows, :] = acc_ref[...].astype(BFLOAT)
    high, low = parts2(den_ref[...])
    blank = jnp.zeros((lines, 128 - QBLOCK), BFLOAT)
    out_ref[rows:, :] = jnp.concatenate([high, blank, low, blank], axis=1)


def gather(me, blk, parts, rows, deps):
    lines = up16(rows // QBLOCK)
    smem = pl.BlockSpec(memory_space=SMEM)
    return pl.pallas_call(
        functools.partial(gather_kernel, len(parts), len(deps)),
        out_shape=VMEM((rows + lines, XHEAD), BFLOAT),
        in_specs=[smem, smem] + whole(len(parts)) + after(len(deps)),
        out_specs=pl.BlockSpec(memory_space=VMEM),
        scratch_shapes=[VMEM((rows, XHEAD), FLOAT32), VMEM((lines, QBLOCK), FLOAT32)],
        compiler_params=GRANT,
        name="gather",
    )(me, blk, *near_core(*parts), *deps)


def combine_kernel(count, deps, head, me_ref, blk_ref, far_ref, *refs):
    parts = refs[:count]
    out_ref, acc_ref, den_ref = refs[count + deps :]
    capacity = blk_ref.shape[1]
    rows = acc_ref.shape[0]
    acc_ref[...] = far_ref[:rows, :].astype(FLOAT32)
    tail = far_ref[rows:, :].astype(FLOAT32)
    den_ref[...] = tail[:, :QBLOCK] + tail[:, 128 : 128 + QBLOCK]
    for k, part_ref in enumerate(parts):
        owner = me_ref[0] ^ k
        add_group([blk_ref[owner, r] for r in range(capacity)], head, part_ref, acc_ref, den_ref)
    turned = jnp.transpose(den_ref[...])
    for b in range(rows // QBLOCK):
        mine = slice(b * QBLOCK, (b + 1) * QBLOCK)
        out_ref[mine, :] = (acc_ref[mine, :] / turned[:, b : b + 1]).astype(BFLOAT)


def combine(me, blk, far, parts, head, rows, deps):
    smem = pl.BlockSpec(memory_space=SMEM)
    return pl.pallas_call(
        functools.partial(combine_kernel, len(parts), len(deps), head),
        out_shape=VMEM((rows, XHEAD), BFLOAT),
        in_specs=[smem, smem] + whole(1 + len(parts)) + after(len(deps)),
        out_specs=pl.BlockSpec(memory_space=VMEM),
        scratch_shapes=[VMEM((rows, XHEAD), FLOAT32),
                        VMEM((far.shape[0] - rows, QBLOCK), FLOAT32)],
        compiler_params=GRANT,
        name="combine",
    )(me, blk, *near_core(far, *parts), *deps)


def gathered_dot(pieces, spots, blocks, me, w_ref):
    total = None
    for (j, h), piece in zip(spots, pieces):
        depth = piece.shape[1]
        rows = pl.ds(pl.multiple_of(((me ^ j) * blocks + h) * depth, depth), depth)
        part = dot(piece[...], w_ref[rows, :])
        total = part if total is None else total + part
    return total


def partial_kernel(spots, blocks, deps, me_ref, *refs):
    *pieces, w_ref = refs[: len(spots) + 1]
    refs[-1][...] = gathered_dot(pieces, spots, blocks, me_ref[0], w_ref)


def final_kernel(spots, blocks, deps, me_ref, *refs):
    *pieces, w_ref, some_ref, gate_ref, mixer_ref = refs[: len(spots) + 4]
    cross = some_ref[...] + gathered_dot(pieces, spots, blocks, me_ref[0], w_ref)
    refs[-1][...] = (mixer_ref[...] + gate_ref[...] * cross).astype(BFLOAT)


def over_tp(body, me, pieces, blocks, others, out, deps=()):
    spots = list(pieces)
    flat = [pieces[spot] for spot in spots]
    return pl.pallas_call(
        functools.partial(body, spots, blocks, len(deps)),
        out_shape=out((flat[0].shape[0], others[0].shape[1])),
        in_specs=[pl.BlockSpec(memory_space=SMEM)] + whole(len(flat) + len(others))
        + after(len(deps)),
        out_specs=pl.BlockSpec(memory_space=VMEM),
        compiler_params=GRANT,
    )(me, *near_core(*flat, *others), *deps)


def gather_tp(piece, count):
    pieces = {0: piece}
    bit = count // 2
    while bit:
        pairs = [(i, i ^ bit) for i in range(count)]
        for j in list(pieces):
            pieces[j ^ bit] = lax.ppermute(pieces[j], "tp", pairs)
        bit //= 2
    return [pieces[j] for j in range(count)]


def local(
    tokens, mix_query, mix_key, mix_value, decay_lower_map, decay_upper_map, decay_base,
    decay_shift, rate_lower_map, rate_upper_map, norm_gain, mix_out, cross_query, score_gain,
    passage_key, passage_value, cross_out, gate_down, gate_up, store, passage_ids,
):
    rows = tokens.shape[0]
    owners = lax.axis_size("st")
    shards = lax.axis_size("tp")
    pass_dev, plen, _ = store.shape
    per_block = passage_ids.shape[1]
    slots = passage_ids.shape[0] * per_block
    capacity = max(2, -(-slots // owners))
    me = lax.axis_index("tp").astype(jnp.int32).reshape(1)
    place = lax.axis_index("st").astype(jnp.int32).reshape(1)
    half = owners // 2

    def swap(value, bit):
        return lax.ppermute(value, "st", [(i, i ^ bit) for i in range(owners)])

    def swap_groups(groups):
        return [groups[0]] + [swap(groups[k], k) for k in range(1, half)]

    blk, queries, near = make_queries(
        place, passage_ids, owners, capacity, pass_dev, tokens, cross_query, score_gain)
    heads = len(queries)
    far_queries = [swap(queries[0], half)]
    near = swap_groups(near)
    keys, values = make_keyvals(store, passage_key, passage_value)
    for q in queries[1:]:
        q, keys = lax.optimization_barrier((q, keys))
        far_queries.append(swap(q, half))
    chunks = rows // MBLOCK
    pieces = [(0, 3), (3, 3), (6, 2)] if chunks == 8 else [(c, 1) for c in range(chunks)]
    prepared = []

    def some_chunks(dep):
        if not pieces:
            return dep
        prepared.append(prepare(mixer_in, *pieces.pop(0), [dep]))
        return prepared[-1][0]

    *mixer_in, gate = project(
        tokens, mix_query, mix_key, mix_value, decay_lower_map, decay_upper_map,
        decay_base, decay_shift, rate_lower_map, rate_upper_map, gate_down, gate_up, [keys])
    last = mixer_in[0]
    far = []
    for h in range(heads):
        far_blk, groups = relay(place, far_queries[h], rows, owners, capacity, [last])
        last = groups[0]
        far.append(swap_groups(groups))
        if h == 0:
            last = some_chunks(last)
    far_parts = []
    for h in range(heads):
        parts = attend(far[h], keys, values, plen, h, [last])
        last = parts[0]
        far_parts.append(swap_groups(parts))
        if h == 0:
            near_parts = attend(near, keys, values, plen, 0, [last])
            last = near_parts[0]
    returned = []
    for h in range(heads):
        sums = gather(place, far_blk, far_parts[h], rows, [last])
        if h == heads - 1:
            near_parts, sums = lax.optimization_barrier((near_parts, sums))
        returned.append(swap(sums, half))
        if h == heads - 1:
            near_parts = swap_groups(near_parts)
        last = some_chunks(sums)
    while pieces:
        last = some_chunks(last)
    mixer_heads = scan(prepared, norm_gain, [])
    mixer_all = gather_tp(mixer_heads, shards)
    last = mixer_heads
    cross = {}
    for h in range(heads):
        last = combine(place, blk, returned[h], near_parts, h, rows, [last])
        for k, piece in enumerate(gather_tp(last, shards)):
            cross[k, h] = piece
    inner = functools.partial(VMEM, dtype=FLOAT32)
    mixer_part = over_tp(partial_kernel, me, {(k, 0): p for k, p in enumerate(mixer_all)}, 1,
                         [mix_out], inner)
    late = [(k, h) for k, h in cross if h == heads - 1 and k > 1]
    some = over_tp(partial_kernel, me, {s: p for s, p in cross.items() if s not in late}, heads,
                   [cross_out], inner, [mixer_part])
    return over_tp(final_kernel, me, {s: cross[s] for s in late}, heads,
                   [cross_out, some, gate, mixer_part],
                   functools.partial(jax.ShapeDtypeStruct, dtype=BFLOAT))


def solution(mesh):
    placed = (
        P("st", None), P(None, "tp"), P(None, "tp"), P(None, "tp"), P(), P(None, "tp"), P("tp"),
        P("st", "tp"), P(), P(None, "tp"), P("tp"), P(None, "tp"), P(None, "tp"), P("tp"),
        P(None, "tp"), P(None, "tp"), P(None, "tp"), P(), P(None, "tp"), P("st", None, None),
        P("st", None),
    )
    return jax.shard_map(
        local, mesh=mesh, in_specs=placed, out_specs=P("st", "tp"), check_vma=False
    )
```

```python
import functools
import jax
import jax.numpy as jnp
from jax import lax
from jax.experimental import pallas as pl
from jax.experimental.pallas import tpu as pltpu
from jax.sharding import PartitionSpec as P


XHEAD = 256
QBLOCK = 64
MBLOCK = 64
RHEAD = 64
LROWS = 8

FLOAT32 = jnp.float32
BFLOAT = jnp.bfloat16
PRECISE = lax.Precision.HIGHEST
VMEM = pltpu.VMEM
SMEM = pltpu.SMEM
GRANT = pltpu.CompilerParams(vmem_limit_bytes=14 * 1024 * 1024)
NT = (((1,), (1,)), ((), ()))
NN = (((1,), (0,)), ((), ()))
TN = (((0,), (0,)), ((), ()))


def dot(left, right, dims=NN, precision=None):
    return lax.dot_general(left, right, dims, precision=precision, preferred_element_type=FLOAT32)


def iota(shape, dim):
    return lax.broadcasted_iota(jnp.int32, shape, dim)


def whole(count):
    return [pl.BlockSpec(memory_space=VMEM)] * count


def in_hbm(*arrays):
    return [pltpu.with_memory_space_constraint(a, pltpu.HBM) for a in arrays]


def near_core(*arrays):
    return [pltpu.with_memory_space_constraint(a, VMEM) for a in arrays]


def after(count):
    return [pl.BlockSpec(memory_space=pl.ANY)] * count


def up8(count):
    return -(-count // 8) * 8


def entry(lines, row, lane):
    hit = (iota(lines.shape, 0) == row) & (iota(lines.shape, 1) == lane)
    return jnp.sum(jnp.where(hit, lines, 0.0)).astype(jnp.int32)


def write_group(out_ref, q_ref, blocks, passages):
    capacity = len(blocks)
    width = out_ref.shape[1]
    line = jnp.zeros((LROWS, width), FLOAT32)
    row, lane = iota(line.shape, 0), iota(line.shape, 1)
    for r in range(capacity):
        start = pl.multiple_of(jnp.maximum(blocks[r] - 1, 0) * QBLOCK, QBLOCK)
        out_ref[r * QBLOCK : (r + 1) * QBLOCK, :] = q_ref[pl.ds(start, QBLOCK), :]
        line = jnp.where((row == 0) & (lane == r), passages[r].astype(FLOAT32), line)
    out_ref[capacity * QBLOCK :, :] = line.astype(BFLOAT)


def query_kernel(pass_dev, owners, me_ref, ids_ref, tok_ref, w_ref, gain_ref, blk_ref, *refs):
    capacity = blk_ref.shape[1]
    per_block = ids_ref.shape[0]
    rows, width = tok_ref.shape[0], w_ref.shape[1]
    heads = width // XHEAD
    q_refs, group_refs = refs[:heads], refs[heads:-4]
    pidx_ref, fill_ref, sum_ref, all_ref = refs[-4:]
    step = pl.program_id(0)

    @pl.when(step == 0)
    def _():
        def clear(o, carry):
            fill_ref[o] = 0
            for r in range(capacity):
                pidx_ref[o, r] = 0
                blk_ref[o, r] = 0
            return carry

        lax.fori_loop(0, owners, clear, 0)

        scale = 65536 // pass_dev + 1

        def put(b, carry):
            for i in range(per_block):
                passage = ids_ref[i, b]
                owner = (passage * scale) >> 16
                rank = fill_ref[owner]
                fill_ref[owner] = rank + 1
                pidx_ref[owner, rank] = passage - owner * pass_dev
                blk_ref[owner, rank] = b + 1
            return carry

        lax.fori_loop(0, ids_ref.shape[1], put, 0)
        sum_ref[...] = jnp.zeros_like(sum_ref)

    sum_ref[...] += dot(tok_ref[...], w_ref[...])

    @pl.when(step == pl.num_programs(0) - 1)
    def _():
        tail = q_refs[0].shape[0] - rows
        row, lane = iota((tail, 128), 0), iota((tail, 128), 1)

        def line(o, table):
            for r in range(capacity):
                table = jnp.where((row == o) & (lane == r), blk_ref[o, r].astype(FLOAT32), table)
                table = jnp.where((row == o) & (lane == capacity + r),
                                  pidx_ref[o, r].astype(FLOAT32), table)
            return table

        table = lax.fori_loop(0, owners, line, jnp.zeros((tail, 128), FLOAT32)).astype(BFLOAT)
        for h, q_ref in enumerate(q_refs):
            cols = slice(h * XHEAD, (h + 1) * XHEAD)
            raw = sum_ref[:, cols]
            scale = lax.rsqrt(jnp.mean(raw * raw, axis=-1, keepdims=True) + 1e-06)
            value = (raw * scale * gain_ref[:, cols]).astype(BFLOAT)
            q_ref[:rows, :] = value
            all_ref[:, cols] = value
            q_ref[rows:, :] = jnp.concatenate([table, jnp.zeros_like(table)], axis=1)
        for k, ref in enumerate(group_refs):
            owner = me_ref[0] ^ k
            write_group(ref, all_ref, [blk_ref[owner, r] for r in range(capacity)],
                        [pidx_ref[owner, r] for r in range(capacity)])


def make_queries(me, ids, owners, capacity, pass_dev, tokens, cross_query, score_gain):
    rows, width = tokens.shape[0], cross_query.shape[1]
    smem = pl.BlockSpec(memory_space=SMEM)
    group = VMEM((capacity * QBLOCK + LROWS, width), BFLOAT)
    count, heads = owners // 2, width // XHEAD
    steps = 4
    depth = tokens.shape[1] // steps
    outs = pl.pallas_call(
        functools.partial(query_kernel, pass_dev, owners),
        grid=(steps,),
        out_shape=[jax.ShapeDtypeStruct((owners, capacity), jnp.int32)]
        + [VMEM((rows + up8(owners), XHEAD), BFLOAT)] * heads + [group] * count,
        in_specs=[smem, smem, pl.BlockSpec((rows, depth), lambda i: (0, i)),
                  pl.BlockSpec((depth, width), lambda i: (i, 0))] + whole(1),
        out_specs=[smem] + whole(heads + count),
        scratch_shapes=[SMEM((owners, capacity), jnp.int32), SMEM((owners,), jnp.int32),
                        VMEM((rows, width), FLOAT32), VMEM((rows, width), BFLOAT)],
        compiler_params=GRANT,
        name="queries",
    )(me, *in_hbm(ids.T, tokens, cross_query, score_gain.reshape(1, -1)))
    return outs[0], outs[1 : 1 + heads], outs[1 + heads :]


def relay_kernel(rows, deps, me_ref, q_ref, *refs):
    blk_ref, *group_refs = refs[deps:]
    _, capacity = blk_ref.shape
    table = q_ref[rows:, :128].astype(FLOAT32)
    for k, ref in enumerate(group_refs):
        owner = me_ref[0] ^ k
        blocks = [entry(table, owner, r) for r in range(capacity)]
        for r in range(capacity):
            blk_ref[owner, r] = blocks[r]
        write_group(ref, q_ref, blocks, [entry(table, owner, capacity + r) for r in range(capacity)])


def relay(me, queries, rows, owners, capacity, deps):
    width = queries.shape[1]
    smem = pl.BlockSpec(memory_space=SMEM)
    group = VMEM((capacity * QBLOCK + LROWS, width), BFLOAT)
    count = owners // 2
    outs = pl.pallas_call(
        functools.partial(relay_kernel, rows, len(deps)),
        out_shape=[jax.ShapeDtypeStruct((owners, capacity), jnp.int32)] + [group] * count,
        in_specs=[smem] + whole(1) + after(len(deps)),
        out_specs=[smem] + whole(count),
        compiler_params=GRANT,
        name="relay",
    )(me, *near_core(queries), *deps)
    return outs[0], outs[1:]


def keyval_kernel(rows_ref, wk_ref, wv_ref, k_ref, v_ref):
    width = wk_ref.shape[1]
    rows = rows_ref[...]
    mine = pl.ds(pl.multiple_of(pl.program_id(0) * rows.shape[0], 16), rows.shape[0])
    for h in range(width // XHEAD):
        cols = slice(h * XHEAD, (h + 1) * XHEAD)
        raw = dot(rows, wk_ref[:, cols])
        scale = lax.rsqrt(jnp.mean(raw * raw, axis=-1, keepdims=True) + 1e-06)
        k_ref[mine, cols] = (raw * scale).astype(BFLOAT)
        v_ref[mine, cols] = dot(rows, wv_ref[:, cols]).astype(BFLOAT)


def make_keyvals(store, passage_key, passage_value):
    pass_dev, plen, model = store.shape
    width = passage_key.shape[1]
    group = max(g for g in range(1, 5) if pass_dev % g == 0)
    tile = group * plen
    shape = VMEM((pass_dev * plen, width), BFLOAT)
    return pl.pallas_call(
        keyval_kernel,
        grid=(pass_dev // group,),
        out_shape=[shape, shape],
        in_specs=[pl.BlockSpec((tile, model), lambda i: (i, 0))] + whole(2),
        out_specs=whole(2),
        compiler_params=GRANT,
        name="keyvals",
    )(*in_hbm(store.reshape(-1, model)), *near_core(passage_key, passage_value))


def project_kernel(
    tok_ref, mq_ref, mk_ref, mv_ref, dl_ref, rl_ref, gd_ref, du_ref, ru_ref, gu_ref,
    base_ref, shift_ref, dep_ref,
    q_ref, k_ref, v_ref, u_ref, rk_ref, lf_ref, gate_ref,
):
    tokens = tok_ref[...]
    width = mq_ref.shape[1]
    rank = dl_ref.shape[0]
    lows = dot(tokens, jnp.concatenate([dl_ref[...], rl_ref[...]], axis=0), NT)
    decay_low = jnp.tanh(lows[:, :rank]).astype(BFLOAT)
    rate_low = lows[:, rank:].astype(BFLOAT)
    gate_low = dot(tokens, gd_ref[...]).astype(BFLOAT)
    gate_ref[...] = jax.nn.sigmoid(dot(gate_low, gu_ref[...]))
    pre = base_ref[...] + dot(decay_low, du_ref[...])
    heads = shift_ref.shape[0]
    owner = (iota((heads, width), 0) == iota((heads, width), 1) // RHEAD).astype(FLOAT32)
    shift = dot(shift_ref[...], owner, TN, precision=PRECISE)
    lf_ref[...] = -jax.nn.sigmoid(pre + shift) * (2.718281828459045 ** -0.5)
    q_ref[...] = dot(tokens, mq_ref[...]).astype(BFLOAT)
    v_ref[...] = dot(tokens, mv_ref[...]).astype(BFLOAT)
    key = dot(tokens, mk_ref[...]).astype(BFLOAT)
    k_ref[...] = key
    key = key.astype(FLOAT32)
    same = (iota((width, width), 0) // RHEAD == iota((width, width), 1) // RHEAD).astype(FLOAT32)
    unit = key * lax.rsqrt(dot(key * key, same, precision=PRECISE) + 1e-06)
    u_ref[...] = unit
    rk_ref[...] = unit * jax.nn.sigmoid(dot(rate_low, ru_ref[...]))


def project(tokens, mix_query, mix_key, mix_value, decay_lower, decay_upper, decay_base,
            decay_shift, rate_lower, rate_upper, gate_down, gate_up, deps):
    rows = tokens.shape[0]
    width = mix_query.shape[1]
    half = VMEM((rows, width), BFLOAT)
    full = VMEM((rows, width), FLOAT32)
    return pl.pallas_call(
        project_kernel,
        out_shape=[half, half, half, full, full, full,
                   VMEM((rows, gate_up.shape[1]), FLOAT32)],
        in_specs=whole(12) + after(len(deps)),
        out_specs=whole(7),
        compiler_params=GRANT,
        name="project",
    )(*near_core(tokens, mix_query, mix_key, mix_value), decay_lower.T, rate_lower.T, gate_down,
      decay_upper, rate_upper, gate_up, decay_base.reshape(1, -1), decay_shift.T, *deps)


def parts2(value):
    high = value.astype(BFLOAT)
    return high, (value - high.astype(FLOAT32)).astype(BFLOAT)


def parts3(value):
    high = value.astype(BFLOAT)
    rest = value - high.astype(FLOAT32)
    return (high,) + parts2(rest)


def spread(value):
    rows, width = value.shape
    lane = iota((1, 128), 1) // RHEAD
    blank = jnp.zeros((rows, 128), value.dtype)
    blocks = []
    for h in range(width // RHEAD):
        mine = (h * RHEAD) // 128
        keep = (lane == h % (128 // RHEAD)).astype(value.dtype)
        cells = [blank] * (width // 128)
        cells[mine] = value[:, mine * 128 : (mine + 1) * 128] * keep
        blocks.append(jnp.concatenate(cells, axis=1) if len(cells) > 1 else cells[0])
    return jnp.concatenate(blocks, axis=0)


def fold(value):
    width = value.shape[1]
    lane = iota((1, 128), 1) // RHEAD
    cells = []
    for t in range(width // 128):
        cell = value[t * 128 : t * 128 + RHEAD, t * 128 : (t + 1) * 128]
        for p in range(1, 128 // RHEAD):
            start = t * 128 + p * RHEAD
            cell = jnp.where(lane == p, value[start : start + RHEAD, t * 128 : (t + 1) * 128], cell)
        cells.append(cell)
    return jnp.concatenate(cells, axis=1) if len(cells) > 1 else cells[0]


def left_of(value):
    high, low = parts2(value)
    return jnp.concatenate([high, low, high], axis=1)


def right_of(value):
    high, low = parts2(value)
    high, low = spread(high), spread(low)
    return jnp.concatenate([high, high, low], axis=0)


def right_nt(value):
    high, low = parts2(value)
    high, low = spread(high), spread(low)
    return jnp.concatenate([high, high, low], axis=1)


def across(left, right):
    lh, ll = parts2(left)
    rh, rl = parts2(right)
    return fold(dot(jnp.concatenate([lh, ll, lh], axis=0), jnp.concatenate([rh, rh, rl], axis=0), TN))


def prepare_chunks(queries, keys, values, units, rate_keys, fades):
    n = range(len(queries))
    length, width = queries[0].shape
    row = iota((length, width), 0)
    col = iota((length, width), 1) % RHEAD
    lower = (iota((length, length), 1) <= iota((length, length), 0)).astype(BFLOAT)
    cumul = []
    for c in n:
        sums = dot(lower, jnp.concatenate(parts3(fades[c]), axis=1))
        cumul.append(sums[:, :width] + sums[:, width : 2 * width] + sums[:, 2 * width :])
    ends = [cumul[c][length - 1 :, :] for c in n]
    grown = [jnp.exp(-cumul[c]) for c in n]
    pulled = [-units[c] * jnp.exp(cumul[c] - fades[c]) for c in n]
    read = [queries[c] * jnp.exp(cumul[c]) for c in n]
    both = [left_of(jnp.concatenate([pulled[c], read[c]], axis=0)) for c in n]
    from_rate = [dot(both[c], right_nt(rate_keys[c] * grown[c]), NT) for c in n]
    from_key = [dot(both[c], right_nt(keys[c] * grown[c]), NT) for c in n]
    strict, upto = col < row, col <= row
    rate_pull = [jnp.where(strict, from_rate[c][:length], 0.0) for c in n]
    rate_read = [left_of(jnp.where(upto, from_rate[c][length:], 0.0)) for c in n]
    key_both = [
        left_of(jnp.concatenate([jnp.where(strict, from_key[c][:length], 0.0),
                                 jnp.where(upto, from_key[c][length:], 0.0)], axis=0)) for c in n]

    def pick(size):
        return (row // (2 * size) == col // (2 * size)) & (row // size > col // size)

    first = pick(1)
    eye = (row == col).astype(FLOAT32)
    inverse = [eye + jnp.where(first, rate_pull[c], 0.0) for c in n]
    size = 2
    while size < length:
        keep = pick(size)
        mids = [dot(left_of(inverse[c]), right_of(jnp.where(keep, rate_pull[c], 0.0))) for c in n]
        adds = [dot(left_of(mids[c]), right_of(inverse[c])) for c in n]
        inverse = [inverse[c] + adds[c] for c in n]
        size *= 2
    inverse = [left_of(inverse[c]) for c in n]
    from_value = []
    for c in n:
        wide = spread(values[c])
        from_value.append(dot(key_both[c][:, : 2 * width], jnp.concatenate([wide, wide], axis=0)))
    moved = [dot(inverse[c], right_of(pulled[c])) for c in n]
    base = [dot(inverse[c], right_of(from_value[c][:length])) for c in n]
    query_end = [read[c] + dot(rate_read[c], right_of(moved[c])) for c in n]
    out_base = [from_value[c][length:] + dot(rate_read[c], right_of(base[c])) for c in n]
    left = [jnp.exp(ends[c] - cumul[c]) for c in n]
    step, add = [], []
    diag = iota((RHEAD, width), 0) == iota((RHEAD, width), 1) % RHEAD
    for c in n:
        rate_left = rate_keys[c] * left[c]
        step.append(jnp.where(diag, jnp.exp(ends[c]), 0.0) + across(moved[c], rate_left))
        add.append(across(jnp.concatenate([values[c].astype(FLOAT32), base[c]], axis=0),
                          jnp.concatenate([keys[c] * left[c], rate_left], axis=0)))
    return query_end, out_base, step, add


def prepare_kernel(start, deps, q_ref, k_ref, v_ref, u_ref, rk_ref, lf_ref, *refs):
    outs = refs[deps:]
    count = outs[0].shape[0] // MBLOCK
    spans = [slice((start + c) * MBLOCK, (start + c + 1) * MBLOCK) for c in range(count)]
    results = prepare_chunks(
        [q_ref[s].astype(FLOAT32) for s in spans], [k_ref[s].astype(FLOAT32) for s in spans],
        [v_ref[s] for s in spans], [u_ref[s] for s in spans], [rk_ref[s] for s in spans],
        [lf_ref[s] for s in spans])
    for ref, values in zip(outs, results):
        for c, value in enumerate(values):
            ref[c * MBLOCK : (c + 1) * MBLOCK] = value


def prepare(inputs, start, count, deps):
    width = inputs[0].shape[1]
    full = VMEM((count * MBLOCK, width), FLOAT32)
    return pl.pallas_call(
        functools.partial(prepare_kernel, start, len(deps)),
        out_shape=[full] * 4,
        in_specs=whole(6) + after(len(deps)),
        out_specs=whole(4),
        compiler_params=GRANT,
        name="prepare",
    )(*near_core(*inputs), *deps)


def head_mean(value, same):
    high, low = parts2(value)
    return dot(jnp.concatenate([high, low], axis=1), same) * (1.0 / RHEAD)


def scan_kernel(deps, pieces, gain_ref, *refs):
    prepared = [refs[4 * p : 4 * p + 4] for p in range(pieces)]
    out_ref, raw_ref = refs[4 * pieces + deps :]
    width = out_ref.shape[1]
    same = (iota((width, width), 0) // RHEAD == iota((width, width), 1) // RHEAD).astype(BFLOAT)
    same = jnp.concatenate([same, same], axis=0)
    state = None
    done = 0
    for qe_ref, ob_ref, st_ref, ad_ref in prepared:
        for c in range(qe_ref.shape[0] // MBLOCK):
            rows = slice(c * MBLOCK, (c + 1) * MBLOCK)
            out = ob_ref[rows, :]
            if state is None:
                state = ad_ref[rows, :]
            else:
                out = out + dot(left_of(qe_ref[rows, :]), right_nt(state), NT)
                state = dot(left_of(state), right_of(st_ref[rows, :])) + ad_ref[rows, :]
            raw_ref[done : done + MBLOCK, :] = out
            done += MBLOCK
    raw = raw_ref[...]
    centred = raw - head_mean(raw, same)
    var = head_mean(centred * centred, same)
    out_ref[...] = (centred * lax.rsqrt(var + 0.00064) * gain_ref[...]).astype(BFLOAT)


def scan(prepared, norm_gain, deps):
    width = prepared[0][0].shape[1]
    rows = sum(p[0].shape[0] for p in prepared)
    flat = [a for p in prepared for a in p]
    return pl.pallas_call(
        functools.partial(scan_kernel, len(deps), len(prepared)),
        out_shape=VMEM((rows, width), BFLOAT),
        in_specs=whole(1 + len(flat)) + after(len(deps)),
        out_specs=pl.BlockSpec(memory_space=VMEM),
        scratch_shapes=[VMEM((rows, width), FLOAT32)],
        compiler_params=GRANT,
        name="scan",
    )(norm_gain.reshape(1, -1), *near_core(*flat), *deps)


def attend_group(plen, first, q_ref, k_ref, v_ref, out_refs):
    width = q_ref.shape[1]
    heads = width // XHEAD
    capacity = (q_ref.shape[0] - LROWS) // QBLOCK
    line = q_ref[capacity * QBLOCK :, :128].astype(FLOAT32)
    units = [(r, h) for r in range(capacity) for h in range(heads)]
    spans = [pl.ds(pl.multiple_of(entry(line, 0, r) * plen, plen), plen) for r in range(capacity)]
    mine = [slice(r * QBLOCK, (r + 1) * QBLOCK) for r in range(capacity)]
    cols = [slice(h * XHEAD, (h + 1) * XHEAD) for h in range(heads)]
    held = [slice((first + h) * XHEAD, (first + h + 1) * XHEAD) for h in range(heads)]
    scores = [dot(q_ref[mine[r], cols[h]], k_ref[spans[r], held[h]], NT) for r, h in units]
    expon = [jnp.exp(s * XHEAD ** (-0.5)).astype(BFLOAT) for s in scores]
    ones = jnp.ones((8, plen), BFLOAT)
    totals = [dot(ones, e, NT)[:1] for e in expon]
    outs = [dot(e, v_ref[spans[r], held[h]]) for e, (r, h) in zip(expon, units)]
    rowid = iota((LROWS, 128), 0)
    sums = [jnp.zeros((LROWS, 128), FLOAT32) for _ in range(heads)]
    blank = jnp.zeros((1, 128 - QBLOCK), FLOAT32)
    for (r, h), out, total in zip(units, outs, totals):
        out_refs[h][mine[r], :] = out.astype(BFLOAT)
        total = jnp.concatenate([total, blank], axis=1)
        high = total.astype(BFLOAT).astype(FLOAT32)
        sums[h] = jnp.where(rowid == 2 * r, high, sums[h])
        sums[h] = jnp.where(rowid == 2 * r + 1, total - high, sums[h])
    for h, out_ref in enumerate(out_refs):
        out_ref[capacity * QBLOCK :, :] = jnp.concatenate([sums[h], sums[h]], axis=1).astype(BFLOAT)


def attend_kernel(plen, first, each, count, deps, k_ref, v_ref, *refs):
    outs = refs[count + deps :]
    for n, q_ref in enumerate(refs[:count]):
        attend_group(plen, first, q_ref, k_ref, v_ref, outs[n * each : (n + 1) * each])


def attend(groups, keys, values, plen, first, deps):
    count = len(groups)
    rows, width = groups[0].shape
    each = width // XHEAD
    outs = pl.pallas_call(
        functools.partial(attend_kernel, plen, first, each, count, len(deps)),
        out_shape=[VMEM((rows, XHEAD), BFLOAT)] * (count * each),
        in_specs=whole(2 + count) + after(len(deps)),
        out_specs=whole(count * each),
        compiler_params=GRANT,
        name="attend",
    )(*near_core(keys, values, *groups), *deps)
    return [outs[h::each] for h in range(each)]


def add_group(blocks, part_ref, acc_ref, den_ref):
    qrows = part_ref.shape[0] - LROWS
    lines = part_ref[qrows:, :QBLOCK].astype(FLOAT32)
    for r, block in enumerate(blocks):
        @pl.when(block > 0)
        def _(r=r, block=block):
            rows = pl.ds(pl.multiple_of((block - 1) * QBLOCK, QBLOCK), QBLOCK)
            acc_ref[rows, :] += part_ref[r * QBLOCK : (r + 1) * QBLOCK, :].astype(FLOAT32)
            den_ref[pl.ds(block - 1, 1), :] += lines[2 * r : 2 * r + 1] + lines[2 * r + 1 : 2 * r + 2]


def gather_kernel(count, deps, me_ref, blk_ref, *refs):
    parts = refs[:count]
    out_ref, acc_ref, den_ref = refs[count + deps :]
    capacity = blk_ref.shape[1]
    acc_ref[...] = jnp.zeros_like(acc_ref)
    den_ref[...] = jnp.zeros_like(den_ref)
    for k, part_ref in enumerate(parts):
        owner = me_ref[0] ^ k
        add_group([blk_ref[owner, r] for r in range(capacity)], part_ref, acc_ref, den_ref)
    rows, lines = acc_ref.shape[0], den_ref.shape[0]
    out_ref[:rows, :] = acc_ref[...].astype(BFLOAT)
    high, low = parts2(den_ref[...])
    blank = jnp.zeros((lines, 128 - QBLOCK), BFLOAT)
    out_ref[rows:, :] = jnp.concatenate([high, blank, low, blank], axis=1)


def gather(me, blk, parts, rows, deps):
    lines = up8(rows // QBLOCK)
    smem = pl.BlockSpec(memory_space=SMEM)
    return pl.pallas_call(
        functools.partial(gather_kernel, len(parts), len(deps)),
        out_shape=VMEM((rows + lines, XHEAD), BFLOAT),
        in_specs=[smem, smem] + whole(len(parts)) + after(len(deps)),
        out_specs=pl.BlockSpec(memory_space=VMEM),
        scratch_shapes=[VMEM((rows, XHEAD), FLOAT32), VMEM((lines, QBLOCK), FLOAT32)],
        compiler_params=GRANT,
        name="gather",
    )(me, blk, *near_core(*parts), *deps)


def combine_kernel(count, deps, me_ref, blk_ref, far_ref, *refs):
    parts = refs[:count]
    out_ref, acc_ref, den_ref = refs[count + deps :]
    capacity = blk_ref.shape[1]
    rows = acc_ref.shape[0]
    acc_ref[...] = far_ref[:rows, :].astype(FLOAT32)
    tail = far_ref[rows:, :].astype(FLOAT32)
    den_ref[...] = tail[:, :QBLOCK] + tail[:, 128 : 128 + QBLOCK]
    for k, part_ref in enumerate(parts):
        owner = me_ref[0] ^ k
        add_group([blk_ref[owner, r] for r in range(capacity)], part_ref, acc_ref, den_ref)
    turned = jnp.transpose(den_ref[...])
    for b in range(rows // QBLOCK):
        mine = slice(b * QBLOCK, (b + 1) * QBLOCK)
        out_ref[mine, :] = (acc_ref[mine, :] / turned[:, b : b + 1]).astype(BFLOAT)


def combine(me, blk, far, parts, rows, deps):
    smem = pl.BlockSpec(memory_space=SMEM)
    return pl.pallas_call(
        functools.partial(combine_kernel, len(parts), len(deps)),
        out_shape=VMEM((rows, XHEAD), BFLOAT),
        in_specs=[smem, smem] + whole(1 + len(parts)) + after(len(deps)),
        out_specs=pl.BlockSpec(memory_space=VMEM),
        scratch_shapes=[VMEM((rows, XHEAD), FLOAT32),
                        VMEM((far.shape[0] - rows, QBLOCK), FLOAT32)],
        compiler_params=GRANT,
        name="combine",
    )(me, blk, *near_core(far, *parts), *deps)


def gathered_dot(pieces, spots, blocks, me, w_ref):
    total = None
    for (j, h), piece in zip(spots, pieces):
        depth = piece.shape[1]
        rows = pl.ds(pl.multiple_of(((me ^ j) * blocks + h) * depth, depth), depth)
        part = dot(piece[...], w_ref[rows, :])
        total = part if total is None else total + part
    return total


def partial_kernel(spots, blocks, deps, me_ref, *refs):
    *pieces, w_ref = refs[: len(spots) + 1]
    refs[-1][...] = gathered_dot(pieces, spots, blocks, me_ref[0], w_ref)


def final_kernel(spots, blocks, deps, me_ref, *refs):
    *pieces, w_ref, some_ref, gate_ref, mixer_ref = refs[: len(spots) + 4]
    cross = some_ref[...] + gathered_dot(pieces, spots, blocks, me_ref[0], w_ref)
    refs[-1][...] = (mixer_ref[...] + gate_ref[...] * cross).astype(BFLOAT)


def over_tp(body, me, pieces, blocks, others, out, deps=()):
    spots = list(pieces)
    flat = [pieces[spot] for spot in spots]
    return pl.pallas_call(
        functools.partial(body, spots, blocks, len(deps)),
        out_shape=out((flat[0].shape[0], others[0].shape[1])),
        in_specs=[pl.BlockSpec(memory_space=SMEM)] + whole(len(flat) + len(others))
        + after(len(deps)),
        out_specs=pl.BlockSpec(memory_space=VMEM),
        compiler_params=GRANT,
    )(me, *near_core(*flat, *others), *deps)


def gather_tp(piece, count):
    pieces = {0: piece}
    bit = count // 2
    while bit:
        pairs = [(i, i ^ bit) for i in range(count)]
        for j in list(pieces):
            pieces[j ^ bit] = lax.ppermute(pieces[j], "tp", pairs)
        bit //= 2
    return [pieces[j] for j in range(count)]


def local(
    tokens, mix_query, mix_key, mix_value, decay_lower_map, decay_upper_map, decay_base,
    decay_shift, rate_lower_map, rate_upper_map, norm_gain, mix_out, cross_query, score_gain,
    passage_key, passage_value, cross_out, gate_down, gate_up, store, passage_ids,
):
    rows = tokens.shape[0]
    owners = lax.axis_size("st")
    shards = lax.axis_size("tp")
    pass_dev, plen, _ = store.shape
    per_block = passage_ids.shape[1]
    slots = passage_ids.shape[0] * per_block
    capacity = max(2, -(-slots // owners))
    me = lax.axis_index("tp").astype(jnp.int32).reshape(1)
    place = lax.axis_index("st").astype(jnp.int32).reshape(1)
    half = owners // 2

    def swap(value, bit):
        return lax.ppermute(value, "st", [(i, i ^ bit) for i in range(owners)])

    def swap_groups(groups):
        return [groups[0]] + [swap(groups[k], k) for k in range(1, half)]

    blk, queries, near = make_queries(
        place, passage_ids, owners, capacity, pass_dev, tokens, cross_query, score_gain)
    heads = len(queries)
    far_queries = [swap(queries[0], half)]
    near = swap_groups(near)
    keys, values = make_keyvals(store, passage_key, passage_value)
    for q in queries[1:]:
        q, keys = lax.optimization_barrier((q, keys))
        far_queries.append(swap(q, half))
    chunks = rows // MBLOCK
    pieces = [(0, 3), (3, 3), (6, 2)] if chunks == 8 else [(c, 1) for c in range(chunks)]
    prepared = []

    def some_chunks(dep):
        if not pieces:
            return dep
        prepared.append(prepare(mixer_in, *pieces.pop(0), [dep]))
        return prepared[-1][0]

    *mixer_in, gate = project(
        tokens, mix_query, mix_key, mix_value, decay_lower_map, decay_upper_map,
        decay_base, decay_shift, rate_lower_map, rate_upper_map, gate_down, gate_up, [keys])
    last = mixer_in[0]
    far = []
    for h in range(heads):
        far_blk, groups = relay(place, far_queries[h], rows, owners, capacity, [last])
        last = groups[0]
        far.append(swap_groups(groups))
        last = some_chunks(last)
    far_parts = []
    for h in range(heads):
        (parts,) = attend(far[h], keys, values, plen, h, [last])
        last = parts[0]
        far_parts.append(swap_groups(parts))
        if h == 0:
            near_parts = attend(near, keys, values, plen, 0, [last])
            last = near_parts[0][0]
    returned = []
    for h in range(heads):
        sums = gather(place, far_blk, far_parts[h], rows, [last])
        if h == heads - 1:
            near_parts, sums = lax.optimization_barrier((near_parts, sums))
        returned.append(swap(sums, half))
        if h == heads - 1:
            near_parts = [
                swap_groups(p)
                for p in near_parts]
        last = some_chunks(sums)
    while pieces:
        last = some_chunks(last)
    mixer_heads = scan(prepared, norm_gain, [])
    mixer_all = gather_tp(mixer_heads, shards)
    last = mixer_heads
    cross = {}
    for h in range(heads):
        last = combine(place, blk, returned[h], near_parts[h], rows, [last])
        for k, piece in enumerate(gather_tp(last, shards)):
            cross[k, h] = piece
    inner = functools.partial(VMEM, dtype=FLOAT32)
    mixer_part = over_tp(partial_kernel, me, {(k, 0): p for k, p in enumerate(mixer_all)}, 1,
                         [mix_out], inner)
    late = [(k, h) for k, h in cross if h == heads - 1 and k > 1]
    some = over_tp(partial_kernel, me, {s: p for s, p in cross.items() if s not in late}, heads,
                   [cross_out], inner, [mixer_part])
    return over_tp(final_kernel, me, {s: cross[s] for s in late}, heads,
                   [cross_out, some, gate, mixer_part],
                   functools.partial(jax.ShapeDtypeStruct, dtype=BFLOAT))


def solution(mesh):
    placed = (
        P("st", None), P(None, "tp"), P(None, "tp"), P(None, "tp"), P(), P(None, "tp"), P("tp"),
        P("st", "tp"), P(), P(None, "tp"), P("tp"), P(None, "tp"), P(None, "tp"), P("tp"),
        P(None, "tp"), P(None, "tp"), P(None, "tp"), P(), P(None, "tp"), P("st", None, None),
        P("st", None),
    )
    return jax.shard_map(
        local, mesh=mesh, in_specs=placed, out_specs=P("st", "tp"), check_vma=False
    )
```
